128 devices in a mesh: sp: 32 (over z, y, core), tp: 4 (over x).
Axes of the slice: x: 4, y: 4, z: 4, core: 2. Of those that a mesh axis runs over, the one named last changes fastest.
Arguments:
- tokens: bfloat16 [12288, 2048], P(('sp', 'tp')), may hold values from -8 to 8, as said below
- query_weight: bfloat16 [2048, 1024], P(None, 'tp'), as said below
- key_weight: bfloat16 [2048, 256], P(None, 'tp'), as said below
- value_weight: bfloat16 [2048, 256], P(None, 'tp'), may hold values from -0.125 to 0.125
- out_weight: bfloat16 [1024, 2048], P('tp'), may hold values from -0.75 to 0.75
- query_gain: bfloat16 [16, 64], P('tp'), may hold values from 0.5 to 6.5
- key_gain: bfloat16 [4, 64], P('tp'), may hold values from 0.5 to 6.5
Outputs:
- mixed: bfloat16 [12288, 2048], P(('sp', 'tp'))
- log_sums: float32 [16, 12288], P('tp', 'sp')
The draws below stay inside these ranges and needn't reach their ends.
Inputs may be any that keep to these rules, and one draw needn't show every extreme that they name: Each block of 384 consecutive tokens has a mean vector of its own. `query_weight`: entries are those of a weight over 2048 inputs, of magnitude at most 6 / sqrt(2048). `key_weight`: entries are those of a weight over 2048 inputs, of magnitude at most 6 / sqrt(2048).
All inputs are finite; a program needn't handle non-finite values.
Results may differ from the reference program's by a relative error of at most 0.028.
Values may be sent and summed in bfloat16 or wider, within the bound.
A program may use at most 64 MiB of HBM per device.

```python
import math
import jax
import jax.numpy as jnp
from jax import lax

D = 2048
HEADS = 16
KV_HEADS = 4
HD = 64
GRID_W = 64
TOK_DEV = 384
TOKENS = 12288
N_TP = 4


def shared_query(key):
    base = jnp.clip(jax.random.normal(jax.random.fold_in(key, 11), (D, HEADS * HD), jnp.float32), -6.0, 6.0)
    base = base * D ** (-0.5)
    return base


def draw_tokens(key, part):
    offsets = jax.random.normal(jax.random.fold_in(key, 21), (TOKENS // TOK_DEV, D), jnp.float32)
    offsets = jnp.repeat(offsets, TOK_DEV, axis=0)
    noise = jax.random.normal(jax.random.fold_in(key, 22), (TOKENS, D), jnp.float32)
    return jnp.clip(noise + offsets, -8.0, 8.0).astype(jnp.bfloat16)


def draw_query_weight(key, part):
    return shared_query(key).astype(jnp.bfloat16)


def draw_key_weight(key, part):
    base = jnp.clip(jax.random.normal(jax.random.fold_in(key, 12), (D, KV_HEADS * HD), jnp.float32), -6.0, 6.0)
    return (base * D ** (-0.5)).astype(jnp.bfloat16)


def draw_query_gain(key, part):
    usual = jax.random.uniform(jax.random.fold_in(key, 31), (HEADS, HD), jnp.float32, 0.5, 1.5)
    return usual.astype(jnp.bfloat16)


def draw_key_gain(key, part):
    return jax.random.uniform(jax.random.fold_in(key, 41), (KV_HEADS, HD), jnp.float32, 0.5, 1.5).astype(jnp.bfloat16)


def level_of(key, shape, shards, low, largest):
    loudness = 1.0
    for dim, blocks in shards:
        draws = jax.random.uniform(jax.random.fold_in(jax.random.fold_in(key, 6), dim), (blocks,), jnp.float32, low / len(shards), largest / len(shards))
        loudness = loudness * jnp.repeat(jnp.exp(draws), shape[dim] // blocks).reshape((-1,) + (1,) * (len(shape) - 1 - dim))
    return loudness


def bell_draw(stream_key, dims, scale, reach, shards=(), held_as=jnp.bfloat16):
    loudness = level_of(stream_key, dims, shards, -0.22, 0.18) if shards else 1.0
    drawn = jax.random.normal(stream_key, dims, jnp.float32) * scale * loudness
    return jnp.minimum(jnp.maximum(drawn, -reach), reach).astype(held_as)


def setup_inputs(seed: int = 0) -> dict:
    key_of = jax.random.split(jax.random.key(seed), 8)
    return {
        "tokens": draw_tokens(jax.random.fold_in(key_of[7], 71), 0),
        "query_weight": draw_query_weight(jax.random.fold_in(key_of[7], 71), 0),
        "key_weight": draw_key_weight(jax.random.fold_in(key_of[7], 71), 0),
        "value_weight": bell_draw(key_of[3], (D, KV_HEADS * HD), D ** -0.5, 0.125, ((1, 4),)),
        "out_weight": bell_draw(key_of[4], (HEADS * HD, D), (HEADS * HD // 16) ** -0.5, 0.75, ((0, 4),)),
        "query_gain": draw_query_gain(jax.random.fold_in(key_of[7], 71), 0),
        "key_gain": draw_key_gain(jax.random.fold_in(key_of[7], 71), 0),
    }


def angle_tables(count):
    quarter = HD // 4
    place = jnp.arange(count, dtype=jnp.int32)
    grid_row = (place // GRID_W).astype(jnp.float32)
    grid_col = (place % GRID_W).astype(jnp.float32)
    freq = 10000.0 ** (-jnp.arange(quarter, dtype=jnp.float32).astype(jnp.float32) / quarter)
    row_angle = grid_row[:, None] * freq[None, :]
    col_angle = grid_col[:, None] * freq[None, :]
    return (jnp.cos(row_angle), jnp.sin(row_angle), jnp.cos(col_angle), jnp.sin(col_angle))

def turn_pairs(part, cosine, sine):
    quarter = part.shape[-1] // 2
    first = part[..., :quarter]
    second = part[..., quarter:]
    cosine = cosine[:, None, :]
    sine = sine[:, None, :]
    return jnp.concatenate([first * cosine - second * sine, second * cosine + first * sine], axis=-1)

def prepare(raw, gain, tables):
    count = raw.shape[0]
    heads = gain.shape[0]
    values = raw.astype(jnp.float32).reshape(count, heads, HD)
    scaled = values * lax.rsqrt(lax.optimization_barrier(jnp.mean(values * values, axis=-1, keepdims=True)) + 1e-06)
    scaled = scaled * gain.astype(jnp.float32)[None, :, :]
    half = HD // 2
    row_cos, row_sin, col_cos, col_sin = tables
    turned = jnp.concatenate([turn_pairs(scaled[..., :half], row_cos, row_sin), turn_pairs(scaled[..., half:], col_cos, col_sin)], axis=-1)
    return turned.astype(jnp.bfloat16)

def reference(tokens, query_weight, key_weight, value_weight, out_weight, query_gain, key_gain):
    count = tokens.shape[0]
    query_raw = jnp.dot(tokens, query_weight, preferred_element_type=jnp.float32).astype(jnp.bfloat16)
    key_raw = jnp.dot(tokens, key_weight, preferred_element_type=jnp.float32).astype(jnp.bfloat16)
    values = jnp.dot(tokens, value_weight, preferred_element_type=jnp.float32).astype(jnp.bfloat16)
    tables = angle_tables(count)
    queries = prepare(query_raw, query_gain, tables)
    keys = prepare(key_raw, key_gain, tables)
    share = HEADS // KV_HEADS
    key_float = keys.astype(jnp.float32)
    value_float = values.reshape(count, KV_HEADS, HD).astype(jnp.float32)
    block_len = math.gcd(count, 128)
    blocks = queries.reshape(count // block_len, block_len, KV_HEADS, share, HD)

    def one_block(query_block):
        scores = jnp.einsum('qhgd,khd->hgqk', query_block.astype(jnp.float32), key_float, precision=lax.Precision.HIGHEST) * HD ** (-0.5)
        row_max = lax.optimization_barrier(jnp.max(scores, axis=-1))
        expo = jnp.exp(scores - row_max[..., None])
        totals = lax.optimization_barrier(jnp.sum(expo, axis=-1))
        weights = lax.optimization_barrier(expo.astype(jnp.bfloat16)).astype(jnp.float32)
        summed = jnp.einsum('hgqk,khd->qhgd', weights, value_float, precision=lax.Precision.HIGHEST)
        attended = summed / jnp.transpose(totals, (2, 0, 1))[..., None]
        log_block = (row_max + jnp.log(totals)).reshape(HEADS, block_len)
        return (attended.astype(jnp.bfloat16).reshape(block_len, HEADS * HD), log_block)
    attended, log_blocks = lax.map(one_block, blocks)
    attended = attended.reshape(count, HEADS * HD)
    log_sums = jnp.transpose(log_blocks, (1, 0, 2)).reshape(HEADS, count)
    group_width = HEADS // N_TP * HD
    total = jnp.zeros((count, D), jnp.float32)
    for group in range(N_TP):
        lo = group * group_width
        partial_sum = jnp.dot(attended[:, lo:lo + group_width], out_weight[lo:lo + group_width], preferred_element_type=jnp.float32).astype(jnp.bfloat16)
        total = total + partial_sum.astype(jnp.float32)
    return (total.astype(jnp.bfloat16), log_sums)
```

```python
import functools
import math

import jax
import jax.numpy as jnp
from jax import lax
from jax.experimental import pallas as pl
from jax.experimental.pallas import tpu as pltpu
from jax.sharding import PartitionSpec as P

MESH = pl.DeviceIdType.MESH
F32 = jnp.float32
BF16 = jnp.bfloat16
NZ, NY, NC, NX = 4, 4, 2, 4
BLK = 96
HALF = 48
D = 2048
HD = 64
HEADS = 4
GRID_W = 64
STAGE_Q = HEADS * BLK
NQ = 4 * STAGE_Q
KC = NY * NC * BLK
QT = 768
VROWS = 80
LOG2E = 1.4426950408889634
LN2 = 0.6931471805599453
OUT_ROWS = 256


def lanes(shape):
    return lax.broadcasted_iota(jnp.int32, shape, 1)


def rows(shape):
    return lax.broadcasted_iota(jnp.int32, shape, 0)


def kernel(
    tok_hbm, wq_hbm, wk_hbm, wv_hbm, wo_hbm, qg_ref, kg_ref,
    out_ref, log_ref,
    toks, wq, wk, wv, wkv, wo, perm, ones, gains, q_rows, kv, vT, sbuf, mnew, acc, mref,
    att_buf, att_in, lrows, local_sem, send_sem, tok_sem, p1_sem, p2_sem, sib_sem, wo_sem, wsib_sem, att_sem,
):
    sp = lax.axis_index("sp")
    tp = lax.axis_index("tp")
    c = lax.rem(sp, 2)
    y = lax.rem(sp // 2, 4)
    z = sp // 8

    def at_zy(zz, yy):
        return ((zz * NY + yy) * NC + c, tp)

    right, left, far = lax.rem(tp + 1, 4), lax.rem(tp + 3, 4), lax.rem(tp + 2, 4)
    sibling = (sp + 1 - 2 * c, tp)
    z_peers = [at_zy(lax.rem(z + d, 4), y) for d in (1, 2, 3)]
    y_peers = [at_zy(z, lax.rem(y + d, 4)) for d in (1, 2, 3)]
    owner = [tp, left, right, far]

    copies = [
        pltpu.make_async_copy(src, dst, local_sem.at[i])
        for i, (src, dst) in enumerate(
            [(tok_hbm, toks.at[0]), (wk_hbm, wk), (wv_hbm, wv), (wq_hbm, wq), (wo_hbm, wo.at[0])]
        )
    ]
    for copy in copies:
        copy.start()

    barrier = pltpu.get_barrier_semaphore()
    peers = [(sp, right), (sp, left), (sp, far), sibling] + z_peers + y_peers
    for peer in peers:
        pl.semaphore_signal(barrier, inc=1, device_id=peer, device_id_type=MESH)

    sends = []

    def send(src, dst, recv, peer):
        copy = pltpu.make_async_remote_copy(
            src_ref=src, dst_ref=dst, send_sem=send_sem.at[len(sends)], recv_sem=recv,
            device_id=peer, device_id_type=MESH,
        )
        sends.append(copy)
        copy.start()
        return copy

    pl.semaphore_wait(barrier, len(peers))
    copies[0].wait()

    halves = (pl.ds(0, HALF), pl.ds(HALF, HALF))
    tok_r, tok_l = [None, None], [None, None]
    for i in (0, 1):
        tok_r[i] = send(toks.at[0, halves[i]], toks.at[1, halves[i]], tok_sem.at[0, i], (sp, right))
        tok_l[1 - i] = send(
            toks.at[0, halves[1 - i]], toks.at[2, halves[1 - i]], tok_sem.at[1, 1 - i], (sp, left)
        )

    i2, j2 = rows((128, 128)), lanes((128, 128))
    lower = (j2 & 31) < 16
    perm[...] = jnp.where(
        lower & (i2 == j2 + 16), -1.0, jnp.where((~lower) & (i2 == j2 - 16), 1.0, 0.0)
    ).astype(BF16)
    ones[...] = jnp.where((i2 // 64) == (j2 // 64), 1.0 / 64.0, 0.0).astype(BF16)
    qg = qg_ref[...].astype(F32)
    kg = kg_ref[...].astype(F32)
    lane1 = lanes((8, 128))
    for g in range(3):
        if g < 2:
            pair = jnp.concatenate([qg[2 * g : 2 * g + 1], qg[2 * g + 1 : 2 * g + 2]], axis=1)
            pair = pair * (HD ** (-0.5) * LOG2E)
        else:
            pair = jnp.concatenate([kg, kg], axis=1)
        pair = jnp.broadcast_to(pair, (8, 128))
        gains[2 * g] = pair
        gains[2 * g + 1] = jnp.where((lane1 & 31) < 16, pltpu.roll(pair, 112, 1), pltpu.roll(pair, 16, 1))

    copies[1].wait()
    copies[2].wait()
    wkv[...] = jnp.concatenate([wk[...], wv[...]], axis=1)
    copies[3].wait()

    lane = lanes((BLK, 128))
    inside = lane & 63
    exponent = (inside & 15).astype(F32) * (-math.log(10000.0) / 16.0)
    freq = jnp.exp(exponent)
    zslot = z

    def project(s):
        place = sp * 384 + owner[s] * BLK + rows((BLK, 128))
        grid_row = (place >> 6).astype(F32)
        grid_col = (place & 63).astype(F32)
        angle = jnp.where(inside < 32, grid_row, grid_col) * freq
        cosine, sine = jnp.cos(angle), jnp.sin(angle)

        def prepare(raw, g):
            value = raw.astype(F32)
            turned = jnp.dot(raw, perm[...], preferred_element_type=F32)
            square = value * value
            high = square.astype(BF16)
            low = (square - high.astype(F32)).astype(BF16)
            mean = jnp.dot(high, ones[...], preferred_element_type=F32) + jnp.dot(
                low, ones[...], preferred_element_type=F32
            )
            inverse = lax.rsqrt(mean + 1e-6)
            return inverse * (
                value * gains[2 * g, 0:1] * cosine + turned * gains[2 * g + 1, 0:1] * sine
            )

        x = toks[s]
        raw = jnp.dot(x, wkv[...], preferred_element_type=F32).astype(BF16)
        slab = jnp.where(lane < 64, prepare(raw, 2), raw.astype(F32))
        kv[4 * s + zslot, y, c] = slab.astype(BF16)
        raw = jnp.dot(x, wq[...], preferred_element_type=F32).astype(BF16)
        for g in range(2):
            done = prepare(raw[:, 128 * g : 128 * g + 128], g)
            q_rows[s, 2 * g] = jnp.where(lane < 64, done, 0.0).astype(BF16)
            q_rows[s, 2 * g + 1] = jnp.where(lane < 64, pltpu.roll(done, 64, 1), 0.0).astype(BF16)

    def phase1(s):
        a = kv.at[4 * s + z, y, c, halves[0]]
        b = kv.at[4 * s + z, y, c, halves[1]]
        first = [send(a, a, p1_sem.at[s, 0, d], z_peers[d]) for d in range(3)]
        return first + [send(b, b, p1_sem.at[s, 1, d], y_peers[d]) for d in range(3)]

    def phase2(s):
        a = kv.at[pl.ds(4 * s, 4), y, c, halves[0]]
        b = kv.at[4 * s + z, :, c, halves[1]]
        first = [send(a, a, p2_sem.at[s, 0, d], y_peers[d]) for d in range(3)]
        return first + [send(b, b, p2_sem.at[s, 1, d], z_peers[d]) for d in range(3)]

    def share(s):
        a = kv.at[pl.ds(4 * s, 4), :, c]
        return [send(a, a, sib_sem.at[s], sibling)]

    def arrive(group):
        for copy in group:
            copy.wait_recv()

    project(0)
    one = {0: phase1(0)}
    two, sib = {}, {}
    arrive([tok_r[0]])
    tok_fr = send(toks.at[1, halves[0]], toks.at[3, halves[0]], tok_sem.at[2, 0], (sp, right))
    arrive([tok_l[1]])
    tok_fl = send(toks.at[2, halves[1]], toks.at[3, halves[1]], tok_sem.at[2, 1], (sp, left))
    arrive(one[0])
    two[0] = phase2(0)
    arrive(two[0])
    sib[0] = share(0)
    arrive([tok_r[1]])
    project(1)
    one[1] = phase1(1)
    arrive([tok_l[0]])
    project(2)
    one[2] = phase1(2)
    arrive(one[1])
    two[1] = phase2(1)
    arrive(one[2])
    two[2] = phase2(2)
    arrive([tok_fr, tok_fl])
    copies[4].wait()
    wo_half = OUT_ROWS // 4
    base = c * (OUT_ROWS // 2)
    wparts = [pl.ds(pl.multiple_of(base + k * wo_half, wo_half), wo_half) for k in (0, 1)]
    wo_r, wo_l = [None, None], [None, None]
    for i in (0, 1):
        wo_r[i] = send(wo.at[0, wparts[i]], wo.at[1, wparts[i]], wo_sem.at[0, i], (sp, right))
        wo_l[1 - i] = send(
            wo.at[0, wparts[1 - i]], wo.at[2, wparts[1 - i]], wo_sem.at[1, 1 - i], (sp, left)
        )
    project(3)
    one[3] = phase1(3)
    arrive(two[1])
    sib[1] = share(1)
    arrive(two[2])
    sib[2] = share(2)
    arrive(one[3])
    two[3] = phase2(3)
    arrive(two[3])
    sib[3] = share(3)
    for s in range(4):
        arrive(sib[s])

    acc[...] = jnp.zeros_like(acc)
    mref[...] = jnp.full_like(mref, -1e30)
    nt = NQ // QT

    def keys_of(n):
        return kv[n].reshape(KC, 128)

    def scores(n, t):
        q = q_rows[pl.ds(t * (QT // STAGE_Q), QT // STAGE_Q)].reshape(QT, 128)
        s = lax.dot_general(keys_of(n), q, (((1,), (1,)), ((), ())), preferred_element_type=F32)
        sbuf[t % 2] = s
        mnew[t % 2, 0:1] = jnp.max(s, axis=0, keepdims=True)

    def make_step(total):
        def step(n, carry):
            following = lax.rem(n + 1, total)
            flipped = keys_of(n).T
            vT[0:64] = flipped[64:128]
            values = vT[...]
            for t in range(nt):
                cols = pl.ds(t * QT, QT)
                if t + 1 < nt:
                    scores(n, t + 1)
                else:
                    scores(following, 0)
                s = sbuf[t % 2]
                old = mref[0:1, cols]
                new = jnp.maximum(old, mnew[t % 2, 0:1])
                weights = jnp.exp2(s - new).astype(BF16)
                factor = jnp.exp2(old - new)
                acc[:, cols] = acc[:, cols] * factor + jnp.dot(
                    values, weights, preferred_element_type=F32
                )
                mref[0:1, cols] = new
            return carry

        return step

    vT[64:VROWS] = jnp.ones((VROWS - 64, KC), BF16)
    scores(0, 0)
    step = make_step(16)
    lax.fori_loop(0, 10, step, 0)
    arrive([wo_r[0]])
    wo_fr = send(wo.at[1, wparts[0]], wo.at[3, wparts[0]], wo_sem.at[2, 0], (sp, right))
    arrive([wo_l[1]])
    wo_fl = send(wo.at[2, wparts[1]], wo.at[3, wparts[1]], wo_sem.at[2, 1], (sp, left))
    arrive([wo_r[1], wo_l[0]])
    whole = pl.ds(pl.multiple_of(base, OUT_ROWS // 2), OUT_ROWS // 2)
    wsib = [send(wo.at[k, whole], wo.at[k, whole], wsib_sem.at[k - 1], sibling) for k in (1, 2)]
    lax.fori_loop(10, 16, step, 0)

    def finish(s):
        part = acc[:, s * STAGE_Q : (s + 1) * STAGE_Q]
        o = (part[0:64] / part[64:65]).T
        for g in range(2):
            att_buf[s, :, 128 * g : 128 * g + 128] = jnp.concatenate(
                [o[2 * g * BLK : (2 * g + 1) * BLK], o[(2 * g + 1) * BLK : (2 * g + 2) * BLK]], axis=1
            ).astype(BF16)

    atts = []
    for s in (3, 1, 2):
        finish(s)
        atts.append(send(att_buf.at[s], att_in.at[s - 1], att_sem.at[s - 1], (sp, owner[s])))
    finish(0)
    arrive([wo_fr, wo_fl])
    wsib.append(send(wo.at[3, whole], wo.at[3, whole], wsib_sem.at[2], sibling))

    logs = (mref[0:1] + jnp.log2(acc[64:65])) * LN2
    tall = jnp.broadcast_to(logs, (128, NQ)).T
    for s in range(4):
        at = pl.ds(pl.multiple_of(owner[s] * BLK, BLK), BLK)
        mixed = jnp.zeros((BLK, 128), F32)
        for h in range(HEADS):
            start = s * STAGE_Q + h * BLK
            mixed = jnp.where(lane == h, tall[start : start + BLK], mixed)
        lrows[at] = mixed
    log_ref[...] = lrows[...].T[0:HEADS]

    arrive(wsib)
    arrive(atts)
    pairs = [(att_buf[0], 0), (att_in[0], 2), (att_in[1], 1), (att_in[2], 3)]
    width = 512
    for n in range(D // width):
        cols = pl.ds(n * width, width)
        total = jnp.zeros((BLK, width), F32)
        for value, slot in pairs:
            total = total + jnp.dot(value, wo[slot, :, cols], preferred_element_type=F32)
        out_ref[:, cols] = total.astype(BF16)

    for copy in sends:
        copy.wait_send()


def body(tokens, query_weight, key_weight, value_weight, out_weight, query_gain, key_gain):
    any_spec = pl.BlockSpec(memory_space=pl.ANY)
    vmem = pl.BlockSpec(memory_space=pltpu.VMEM)
    dma = pltpu.SemaphoreType.DMA
    return pl.pallas_call(
        kernel,
        out_shape=(
            jax.ShapeDtypeStruct((BLK, D), BF16),
            jax.ShapeDtypeStruct((HEADS, 4 * BLK), F32),
        ),
        in_specs=[any_spec] * 5 + [vmem] * 2,
        out_specs=(vmem, vmem),
        scratch_shapes=[
            pltpu.VMEM((4, BLK, D), BF16),
            pltpu.VMEM((D, 256), BF16),
            pltpu.VMEM((D, 64), BF16),
            pltpu.VMEM((D, 64), BF16),
            pltpu.VMEM((D, 128), BF16),
            pltpu.VMEM((4, OUT_ROWS, D), BF16),
            pltpu.VMEM((128, 128), BF16),
            pltpu.VMEM((128, 128), BF16),
            pltpu.VMEM((6, 8, 128), F32),
            pltpu.VMEM((4, HEADS, BLK, 128), BF16),
            pltpu.VMEM((16, NY, NC, BLK, 128), BF16),
            pltpu.VMEM((VROWS, KC), BF16),
            pltpu.VMEM((2, KC, QT), F32),
            pltpu.VMEM((2, 8, QT), F32),
            pltpu.VMEM((VROWS, NQ), F32),
            pltpu.VMEM((8, NQ), F32),
            pltpu.VMEM((4, BLK, 256), BF16),
            pltpu.VMEM((3, BLK, 256), BF16),
            pltpu.VMEM((4 * BLK, 128), F32),
            dma((5,)),
            dma((80,)),
            dma((3, 2)),
            dma((4, 2, 3)),
            dma((4, 2, 3)),
            dma((4,)),
            dma((3, 2)),
            dma((3,)),
            dma((3,)),
        ],
        compiler_params=pltpu.CompilerParams(
            collective_id=0, has_side_effects=True, vmem_limit_bytes=60 * 2**20
        ),
    )(tokens, query_weight, key_weight, value_weight, out_weight, query_gain, key_gain)


def solution(mesh):
    return jax.shard_map(
        body,
        mesh=mesh,
        in_specs=(
            P(("sp", "tp"), None),
            P(None, "tp"),
            P(None, "tp"),
            P(None, "tp"),
            P("tp", None),
            P("tp", None),
            P("tp", None),
        ),
        out_specs=(P(("sp", "tp"), None), P("tp", "sp")),
        check_vma=False,
    )
```

```python
import functools
import math

import jax
import jax.numpy as jnp
from jax import lax
from jax.experimental import pallas as pl
from jax.experimental.pallas import tpu as pltpu
from jax.sharding import PartitionSpec as P

MESH = pl.DeviceIdType.MESH
F32 = jnp.float32
BF16 = jnp.bfloat16
NZ, NY, NC, NX = 4, 4, 2, 4
BLK = 96
HALF = 48
D = 2048
HD = 64
HEADS = 4
GRID_W = 64
STAGE_Q = HEADS * BLK
NQ = 4 * STAGE_Q
KC = NY * NC * BLK
QT = 768
VROWS = 80
LOG2E = 1.4426950408889634
LN2 = 0.6931471805599453
OUT_ROWS = 256


def lanes(shape):
    return lax.broadcasted_iota(jnp.int32, shape, 1)


def rows(shape):
    return lax.broadcasted_iota(jnp.int32, shape, 0)


def kernel(
    tok_hbm, wq_hbm, wk_hbm, wv_hbm, wo_hbm, qg_ref, kg_ref,
    out_ref, log_ref,
    toks, wq, wkv, wo, perm, ones, gains, q_rows, kv, vT, sbuf, mnew, acc, mref,
    att_buf, att_in, lrows, local_sem, send_sem, tok_sem, p1_sem, p2_sem, sib_sem, wo_sem, wsib_sem, att_sem,
):
    sp = lax.axis_index("sp")
    tp = lax.axis_index("tp")
    c = lax.rem(sp, 2)
    y = lax.rem(sp // 2, 4)
    z = sp // 8

    def at_zy(zz, yy):
        return ((zz * NY + yy) * NC + c, tp)

    right, left, far = lax.rem(tp + 1, 4), lax.rem(tp + 3, 4), lax.rem(tp + 2, 4)
    sibling = (sp + 1 - 2 * c, tp)
    z_peers = [at_zy(lax.rem(z + d, 4), y) for d in (1, 2, 3)]
    y_peers = [at_zy(z, lax.rem(y + d, 4)) for d in (1, 2, 3)]
    owner = [tp, left, right, far]

    copies = [
        pltpu.make_async_copy(src, dst, local_sem.at[i])
        for i, (src, dst) in enumerate(
            [
                (tok_hbm, toks.at[0]), (wk_hbm, wkv.at[pl.ds(0, HD)]), (wv_hbm, wkv.at[pl.ds(HD, HD)]),
                (wq_hbm, wq), (wo_hbm, wo.at[0]),
            ]
        )
    ]
    for copy in copies:
        copy.start()

    barrier = pltpu.get_barrier_semaphore()
    peers = [(sp, right), (sp, left), (sp, far), sibling] + z_peers + y_peers
    for peer in peers:
        pl.semaphore_signal(barrier, inc=1, device_id=peer, device_id_type=MESH)

    sends = []

    def send(src, dst, recv, peer):
        copy = pltpu.make_async_remote_copy(
            src_ref=src, dst_ref=dst, send_sem=send_sem.at[len(sends)], recv_sem=recv,
            device_id=peer, device_id_type=MESH,
        )
        sends.append(copy)
        copy.start()
        return copy

    i2, j2 = rows((128, 128)), lanes((128, 128))
    lower = (j2 & 31) < 16
    perm[...] = jnp.where(
        lower & (i2 == j2 + 16), -1.0, jnp.where((~lower) & (i2 == j2 - 16), 1.0, 0.0)
    ).astype(BF16)
    ones[...] = jnp.where((i2 // 64) == (j2 // 64), 1.0 / 64.0, 0.0).astype(BF16)
    qg = qg_ref[...].astype(F32)
    kg = kg_ref[...].astype(F32)
    lane1 = lanes((8, 128))
    for g in range(3):
        if g < 2:
            pair = jnp.concatenate([qg[2 * g : 2 * g + 1], qg[2 * g + 1 : 2 * g + 2]], axis=1)
            pair = pair * (HD ** (-0.5) * LOG2E)
        else:
            pair = jnp.concatenate([kg, kg], axis=1)
        pair = jnp.broadcast_to(pair, (8, 128))
        gains[2 * g] = pair
        gains[2 * g + 1] = jnp.where((lane1 & 31) < 16, pltpu.roll(pair, 112, 1), pltpu.roll(pair, 16, 1))

    pl.semaphore_wait(barrier, len(peers))
    copies[0].wait()
    halves = (pl.ds(0, HALF), pl.ds(HALF, HALF))
    tok_r, tok_l = [None, None], [None, None]
    for i in (0, 1):
        tok_r[i] = send(toks.at[0, halves[i]], toks.at[1 + i, halves[0]], tok_sem.at[0, i], (sp, right))
        tok_l[1 - i] = send(
            toks.at[0, halves[1 - i]], toks.at[1 + i, halves[1]], tok_sem.at[1, 1 - i], (sp, left)
        )
    for copy in copies[1:4]:
        copy.wait()

    lane = lanes((BLK, 128))
    inside = lane & 63
    exponent = (inside & 15).astype(F32) * (-math.log(10000.0) / 16.0)
    freq = jnp.exp(exponent)
    zslot = z

    def project(s):
        within = rows((BLK, 128))
        if s == 1:
            place = jnp.where(within < HALF, left * BLK, right * BLK) + within
        elif s == 2:
            place = jnp.where(within < HALF, left * BLK + HALF, right * BLK - HALF) + within
        else:
            place = owner[s] * BLK + within
        place = sp * 384 + place
        grid_row = (place >> 6).astype(F32)
        grid_col = (place & 63).astype(F32)
        angle = jnp.where(inside < 32, grid_row, grid_col) * freq
        cosine, sine = jnp.cos(angle), jnp.sin(angle)

        def prepare(raw, g):
            value = raw.astype(F32)
            turned = jnp.dot(raw, perm[...], preferred_element_type=F32)
            square = value * value
            high = square.astype(BF16)
            low = (square - high.astype(F32)).astype(BF16)
            mean = jnp.dot(high, ones[...], preferred_element_type=F32) + jnp.dot(
                low, ones[...], preferred_element_type=F32
            )
            inverse = lax.rsqrt(mean + 1e-6)
            return inverse * (
                value * gains[2 * g, 0:1] * cosine + turned * gains[2 * g + 1, 0:1] * sine
            )

        x = toks[s]
        raw = lax.dot_general(
            x, wkv[...], (((1,), (1,)), ((), ())), preferred_element_type=F32
        ).astype(BF16)
        slab = jnp.where(lane < 64, prepare(raw, 2), raw.astype(F32))
        kv[4 * s + zslot, y, c] = slab.astype(BF16)
        raw = jnp.dot(x, wq[...], preferred_element_type=F32).astype(BF16)
        for g in range(2):
            done = prepare(raw[:, 128 * g : 128 * g + 128], g)
            q_rows[s, 2 * g] = jnp.where(lane < 64, done, 0.0).astype(BF16)
            q_rows[s, 2 * g + 1] = jnp.where(lane < 64, pltpu.roll(done, 64, 1), 0.0).astype(BF16)

    def phase1(s):
        a = kv.at[4 * s + z, y, c, halves[0]]
        b = kv.at[4 * s + z, y, c, halves[1]]
        first = [send(a, a, p1_sem.at[s, 0, d], z_peers[d]) for d in range(3)]
        return first + [send(b, b, p1_sem.at[s, 1, d], y_peers[d]) for d in range(3)]

    def phase2(s):
        a = kv.at[pl.ds(4 * s, 4), y, c, halves[0]]
        b = kv.at[4 * s + z, :, c, halves[1]]
        first = [send(a, a, p2_sem.at[s, 0, d], y_peers[d]) for d in range(3)]
        return first + [send(b, b, p2_sem.at[s, 1, d], z_peers[d]) for d in range(3)]

    def share(s):
        a = kv.at[pl.ds(4 * s, 4), :, c]
        return [send(a, a, sib_sem.at[s], sibling)]

    def arrive(group):
        for copy in group:
            copy.wait_recv()

    acc[...] = jnp.zeros_like(acc)
    mref[...] = jnp.full_like(mref, -1e30)
    vT[:, HD:VROWS] = jnp.ones((2, VROWS - HD, KC), BF16)
    per_tile = QT // STAGE_Q

    def keys_of(n):
        return kv[n].reshape(KC, 128)

    def scores(n, t, slot):
        q = q_rows[pl.ds(t * per_tile, per_tile)].reshape(QT, 128)
        s = lax.dot_general(keys_of(n), q, (((1,), (1,)), ((), ())), preferred_element_type=F32)
        sbuf[slot] = s
        mnew[slot, 0:1] = jnp.max(s, axis=0, keepdims=True)

    def weigh(t, slot, values):
        cols = pl.ds(t * QT, QT)
        old = mref[0:1, cols]
        new = jnp.maximum(old, mnew[slot, 0:1])
        weights = jnp.exp2(sbuf[slot] - new).astype(BF16)
        factor = jnp.exp2(old - new)
        acc[:, cols] = acc[:, cols] * factor + jnp.dot(values, weights, preferred_element_type=F32)
        mref[0:1, cols] = new

    def values_of(n, slot):
        flipped = keys_of(n).T
        vT[slot, 0:HD] = flipped[HD:128]
        return vT[slot]

    def attend(first, count, tile):
        def step(k, carry):
            n = first + 2 * k
            values = values_of(n, 0)
            scores(n + 1, tile, 1)
            weigh(tile, 0, values)
            values = values_of(n + 1, 1)
            scores(first + lax.rem(2 * k + 2, count), tile, 0)
            weigh(tile, 1, values)
            return carry

        scores(first, tile, 0)
        lax.fori_loop(0, count // 2, step, 0)

    def finish(s):
        part = acc[:, s * STAGE_Q : (s + 1) * STAGE_Q]
        o = (part[0:HD] / part[HD : HD + 1]).T
        for g in range(2):
            att_buf[s, :, 128 * g : 128 * g + 128] = jnp.concatenate(
                [o[2 * g * BLK : (2 * g + 1) * BLK], o[(2 * g + 1) * BLK : (2 * g + 2) * BLK]], axis=1
            ).astype(BF16)

    project(0)
    one0 = phase1(0)
    arrive(one0)
    two0 = phase2(0)
    arrive([tok_r[0]])
    tok_fr = send(toks.at[1, halves[0]], toks.at[3, halves[0]], tok_sem.at[2, 0], (sp, right))
    arrive([tok_l[1]])
    tok_fl = send(toks.at[1, halves[1]], toks.at[3, halves[1]], tok_sem.at[2, 1], (sp, left))
    project(1)
    one1 = phase1(1)
    arrive(two0)
    sib0 = share(0)
    arrive(one1)
    two1 = phase2(1)
    arrive([tok_r[1], tok_l[0]])
    project(2)
    one2 = phase1(2)
    arrive(sib0)
    attend(0, 4, 0)
    arrive(one2)
    two2 = phase2(2)
    arrive(two1)
    sib1 = share(1)
    arrive([tok_fr, tok_fl])
    copies[4].wait()
    wo_half = OUT_ROWS // 4
    base = c * (OUT_ROWS // 2)
    wparts = [pl.ds(pl.multiple_of(base + k * wo_half, wo_half), wo_half) for k in (0, 1)]
    wo_r, wo_l = [None, None], [None, None]
    for i in (0, 1):
        wo_r[i] = send(wo.at[0, wparts[i]], wo.at[1, wparts[i]], wo_sem.at[0, i], (sp, right))
        wo_l[1 - i] = send(
            wo.at[0, wparts[1 - i]], wo.at[2, wparts[1 - i]], wo_sem.at[1, 1 - i], (sp, left)
        )
    project(3)
    one3 = phase1(3)
    arrive(sib1)
    attend(4, 4, 0)
    arrive(one3)
    two3 = phase2(3)
    arrive(two2)
    sib2 = share(2)
    attend(0, 8, 1)
    arrive([wo_r[0]])
    wo_fr = send(wo.at[1, wparts[0]], wo.at[3, wparts[0]], wo_sem.at[2, 0], (sp, right))
    arrive([wo_l[1]])
    wo_fl = send(wo.at[2, wparts[1]], wo.at[3, wparts[1]], wo_sem.at[2, 1], (sp, left))
    arrive(two3)
    sib3 = share(3)
    arrive(sib2)
    arrive(sib3)
    attend(8, 8, 1)
    finish(2)
    finish(3)

    def hand_over(s, half, slot, into, sem, peer):
        return send(att_buf.at[s, halves[half]], att_in.at[slot, halves[into]], att_sem.at[sem], peer)

    atts = [
        hand_over(2, 0, 0, 1, 0, (sp, left)),
        hand_over(2, 1, 1, 0, 1, (sp, right)),
        send(att_buf.at[3], att_in.at[2], att_sem.at[2], (sp, far)),
    ]
    arrive([wo_r[1], wo_l[0]])
    whole = pl.ds(pl.multiple_of(base, OUT_ROWS // 2), OUT_ROWS // 2)
    wsib = [send(wo.at[k, whole], wo.at[k, whole], wsib_sem.at[k - 1], sibling) for k in (1, 2)]
    attend(8, 8, 0)
    finish(1)
    atts.append(hand_over(1, 0, 0, 0, 3, (sp, left)))
    atts.append(hand_over(1, 1, 1, 1, 4, (sp, right)))
    finish(0)
    arrive([wo_fr, wo_fl])
    wsib.append(send(wo.at[3, whole], wo.at[3, whole], wsib_sem.at[2], sibling))

    logs = (mref[0:1] + jnp.log2(acc[64:65])) * LN2
    tall = jnp.broadcast_to(logs, (128, NQ)).T
    places = [
        (0, tp * BLK), (HALF, tp * BLK + HALF), (0, left * BLK), (HALF, right * BLK + HALF),
        (0, left * BLK + HALF), (HALF, right * BLK), (0, far * BLK), (HALF, far * BLK + HALF),
    ]
    for k, (inner, place) in enumerate(places):
        mixed = jnp.zeros((HALF, 128), F32)
        for h in range(HEADS):
            start = (k // 2) * STAGE_Q + h * BLK + inner
            mixed = jnp.where(lane[0:HALF] == h, tall[start : start + HALF], mixed)
        lrows[pl.ds(pl.multiple_of(place, HALF), HALF)] = mixed
    log_ref[...] = lrows[...].T[0:HEADS]

    arrive(wsib)
    arrive(atts)
    pairs = [(att_buf[0], 0), (att_in[0], 2), (att_in[1], 1), (att_in[2], 3)]
    width = 512
    for n in range(D // width):
        cols = pl.ds(n * width, width)
        total = jnp.zeros((BLK, width), F32)
        for value, slot in pairs:
            total = total + jnp.dot(value, wo[slot, :, cols], preferred_element_type=F32)
        out_ref[:, cols] = total.astype(BF16)

    for copy in sends:
        copy.wait_send()


def body(tokens, query_weight, key_weight, value_weight, out_weight, query_gain, key_gain):
    any_spec = pl.BlockSpec(memory_space=pl.ANY)
    vmem = pl.BlockSpec(memory_space=pltpu.VMEM)
    dma = pltpu.SemaphoreType.DMA
    return pl.pallas_call(
        kernel,
        out_shape=(
            jax.ShapeDtypeStruct((BLK, D), BF16),
            jax.ShapeDtypeStruct((HEADS, 4 * BLK), F32),
        ),
        in_specs=[any_spec] * 5 + [vmem] * 2,
        out_specs=(vmem, vmem),
        scratch_shapes=[
            pltpu.VMEM((4, BLK, D), BF16),
            pltpu.VMEM((D, 256), BF16),
            pltpu.VMEM((128, D), BF16),
            pltpu.VMEM((4, OUT_ROWS, D), BF16),
            pltpu.VMEM((128, 128), BF16),
            pltpu.VMEM((128, 128), BF16),
            pltpu.VMEM((6, 8, 128), F32),
            pltpu.VMEM((4, HEADS, BLK, 128), BF16),
            pltpu.VMEM((16, NY, NC, BLK, 128), BF16),
            pltpu.VMEM((2, VROWS, KC), BF16),
            pltpu.VMEM((2, KC, QT), F32),
            pltpu.VMEM((2, 8, QT), F32),
            pltpu.VMEM((VROWS, NQ), F32),
            pltpu.VMEM((8, NQ), F32),
            pltpu.VMEM((4, BLK, 256), BF16),
            pltpu.VMEM((3, BLK, 256), BF16),
            pltpu.VMEM((4 * BLK, 128), F32),
            dma((5,)),
            dma((80,)),
            dma((3, 2)),
            dma((4, 2, 3)),
            dma((4, 2, 3)),
            dma((4,)),
            dma((3, 2)),
            dma((3,)),
            dma((5,)),
        ],
        compiler_params=pltpu.CompilerParams(
            collective_id=0, has_side_effects=True, vmem_limit_bytes=60 * 2**20
        ),
    )(tokens, query_weight, key_weight.T, value_weight.T, out_weight, query_gain, key_gain)


def solution(mesh):
    return jax.shard_map(
        body,
        mesh=mesh,
        in_specs=(
            P(("sp", "tp"), None),
            P(None, "tp"),
            P(None, "tp"),
            P(None, "tp"),
            P("tp", None),
            P("tp", None),
            P("tp", None),
        ),
        out_specs=(P(("sp", "tp"), None), P("tp", "sp")),
        check_vma=False,
    )
```

```python
import functools
import math

import jax
import jax.numpy as jnp
from jax import lax
from jax.experimental import pallas as pl
from jax.experimental.pallas import tpu as pltpu
from jax.sharding import PartitionSpec as P

MESH = pl.DeviceIdType.MESH
F32 = jnp.float32
BF16 = jnp.bfloat16
NZ, NY, NC, NX = 4, 4, 2, 4
BLK = 96
HALF = 48
D = 2048
HD = 64
HEADS = 4
GRID_W = 64
STAGE_Q = HEADS * BLK
NQ = 4 * STAGE_Q
KC = NY * NC * BLK
QT = 768
VROWS = 80
LOG2E = 1.4426950408889634
LN2 = 0.6931471805599453
ORDER = [(0, 0, r) for r in range(4)] + [(0, 1, 0), (0, 1, 1)] + [(1, 0, r) for r in range(4)]
ORDER += [(0, 1, 2), (0, 1, 3)] + [(1, 1, r) for r in range(4)]
ORDER += [(t, s, r) for s in (2, 3) for t in (1, 0) for r in range(4)]
OUT_ROWS = 256


def lanes(shape):
    return lax.broadcasted_iota(jnp.int32, shape, 1)


def rows(shape):
    return lax.broadcasted_iota(jnp.int32, shape, 0)


def kernel(
    tok_hbm, wq_hbm, wk_hbm, wv_hbm, wo_hbm, qg_ref, kg_ref,
    out_ref, log_ref,
    toks, wq, wkv, wo, perm, ones, gains, q_rows, kv, vT, sbuf, mnew, acc, mref,
    att_buf, att_in, lrows, local_sem, send_sem, tok_sem, p1_sem, p2_sem, sib_sem, wo_sem, wsib_sem, att_sem,
):
    sp = lax.axis_index("sp")
    tp = lax.axis_index("tp")
    c = lax.rem(sp, 2)
    y = lax.rem(sp // 2, 4)
    z = sp // 8

    def at_zy(zz, yy):
        return ((zz * NY + yy) * NC + c, tp)

    right, left, far = lax.rem(tp + 1, 4), lax.rem(tp + 3, 4), lax.rem(tp + 2, 4)
    sibling = (sp + 1 - 2 * c, tp)
    z_peers = [at_zy(lax.rem(z + d, 4), y) for d in (1, 2, 3)]
    y_peers = [at_zy(z, lax.rem(y + d, 4)) for d in (1, 2, 3)]
    owner = [tp, left, right, far]

    copies = [
        pltpu.make_async_copy(src, dst, local_sem.at[i])
        for i, (src, dst) in enumerate(
            [
                (tok_hbm, toks.at[0]), (wk_hbm, wkv.at[pl.ds(0, HD)]), (wv_hbm, wkv.at[pl.ds(HD, HD)]),
                (wq_hbm, wq), (wo_hbm, wo.at[0]),
            ]
        )
    ]
    for copy in copies:
        copy.start()

    barrier = pltpu.get_barrier_semaphore()
    peers = [(sp, right), (sp, left), (sp, far), sibling] + z_peers + y_peers
    for peer in peers:
        pl.semaphore_signal(barrier, inc=1, device_id=peer, device_id_type=MESH)

    sends = []

    def send(src, dst, recv, peer):
        copy = pltpu.make_async_remote_copy(
            src_ref=src, dst_ref=dst, send_sem=send_sem.at[len(sends)], recv_sem=recv,
            device_id=peer, device_id_type=MESH,
        )
        sends.append(copy)
        copy.start()
        return copy

    i2, j2 = rows((128, 128)), lanes((128, 128))
    lower = (j2 & 31) < 16
    perm[...] = jnp.where(
        lower & (i2 == j2 + 16), -1.0, jnp.where((~lower) & (i2 == j2 - 16), 1.0, 0.0)
    ).astype(BF16)
    ones[...] = jnp.where((i2 // 64) == (j2 // 64), 1.0 / 64.0, 0.0).astype(BF16)
    qg = qg_ref[...].astype(F32)
    kg = kg_ref[...].astype(F32)
    lane1 = lanes((8, 128))
    for g in range(3):
        if g < 2:
            pair = jnp.concatenate([qg[2 * g : 2 * g + 1], qg[2 * g + 1 : 2 * g + 2]], axis=1)
            pair = pair * (HD ** (-0.5) * LOG2E)
        else:
            pair = jnp.concatenate([kg, kg], axis=1)
        pair = jnp.broadcast_to(pair, (8, 128))
        gains[2 * g] = pair
        gains[2 * g + 1] = jnp.where((lane1 & 31) < 16, pltpu.roll(pair, 112, 1), pltpu.roll(pair, 16, 1))

    pl.semaphore_wait(barrier, len(peers))
    copies[0].wait()
    halves = (pl.ds(0, HALF), pl.ds(HALF, HALF))
    tok_r, tok_l = [None, None], [None, None]
    for i in (0, 1):
        tok_r[i] = send(toks.at[0, halves[i]], toks.at[1 + i, halves[0]], tok_sem.at[0, i], (sp, right))
        tok_l[1 - i] = send(
            toks.at[0, halves[1 - i]], toks.at[1 + i, halves[1]], tok_sem.at[1, 1 - i], (sp, left)
        )
    for copy in copies[1:4]:
        copy.wait()

    lane = lanes((BLK, 128))
    inside = lane & 63
    exponent = (inside & 15).astype(F32) * (-math.log(10000.0) / 16.0)
    freq = jnp.exp(exponent)

    def project(s):
        within = rows((BLK, 128))
        if s == 1:
            place = jnp.where(within < HALF, left * BLK, right * BLK) + within
        elif s == 2:
            place = jnp.where(within < HALF, left * BLK + HALF, right * BLK - HALF) + within
        else:
            place = owner[s] * BLK + within
        place = sp * 384 + place
        grid_row = (place >> 6).astype(F32)
        grid_col = (place & 63).astype(F32)
        angle = jnp.where(inside < 32, grid_row, grid_col) * freq
        cosine, sine = jnp.cos(angle), jnp.sin(angle)

        def prepare(raw, g):
            value = raw.astype(F32)
            turned = jnp.dot(raw, perm[...], preferred_element_type=F32)
            square = value * value
            high = square.astype(BF16)
            low = (square - high.astype(F32)).astype(BF16)
            mean = jnp.dot(high, ones[...], preferred_element_type=F32) + jnp.dot(
                low, ones[...], preferred_element_type=F32
            )
            inverse = lax.rsqrt(mean + 1e-6)
            return inverse * (
                value * gains[2 * g, 0:1] * cosine + turned * gains[2 * g + 1, 0:1] * sine
            )

        x = toks[s]
        raw = lax.dot_general(
            x, wkv[...], (((1,), (1,)), ((), ())), preferred_element_type=F32
        ).astype(BF16)
        slab = jnp.where(lane < 64, prepare(raw, 2), raw.astype(F32))
        kv[c, 4 * s + z, y] = slab.astype(BF16)
        raw = jnp.dot(x, wq[...], preferred_element_type=F32).astype(BF16)
        for g in range(2):
            done = prepare(raw[:, 128 * g : 128 * g + 128], g)
            q_rows[s, 2 * g] = jnp.where(lane < 64, done, 0.0).astype(BF16)
            q_rows[s, 2 * g + 1] = jnp.where(lane < 64, pltpu.roll(done, 64, 1), 0.0).astype(BF16)

    def phase1(s):
        a = kv.at[c, 4 * s + z, y, halves[0]]
        b = kv.at[c, 4 * s + z, y, halves[1]]
        first = [send(a, a, p1_sem.at[s, 0, d], z_peers[d]) for d in range(3)]
        return first + [send(b, b, p1_sem.at[s, 1, d], y_peers[d]) for d in range(3)]

    def phase2(s):
        a = kv.at[c, pl.ds(4 * s, 4), y, halves[0]]
        b = kv.at[c, 4 * s + z, :, halves[1]]
        first = [send(a, a, p2_sem.at[s, 0, d], y_peers[d]) for d in range(3)]
        return first + [send(b, b, p2_sem.at[s, 1, d], z_peers[d]) for d in range(3)]

    def share(s):
        a = kv.at[c, pl.ds(4 * s, 4)]
        return [send(a, a, sib_sem.at[s], sibling)]

    def arrive(group):
        for copy in group:
            copy.wait_recv()

    acc[...] = jnp.zeros_like(acc)
    mref[...] = jnp.full_like(mref, -1e30)
    vT[:, HD:VROWS] = jnp.ones((2, VROWS - HD, KC), BF16)
    per_tile = QT // STAGE_Q

    def keys_of(i):
        s, r = ORDER[i][1:]
        core = lax.rem(c + r // 2, 2)
        place = 4 * s + 2 * (r % 2)
        return kv[core, place : place + 2].reshape(KC, 128)

    def scores(i):
        tile, slot = ORDER[i][0], i % 2
        q = q_rows[tile * per_tile : (tile + 1) * per_tile].reshape(QT, 128)
        s = lax.dot_general(keys_of(i), q, (((1,), (1,)), ((), ())), preferred_element_type=F32)
        sbuf[slot] = s
        mnew[slot, 0:1] = jnp.max(s, axis=0, keepdims=True)

    def weigh(i):
        tile, slot = ORDER[i][0], i % 2
        flipped = keys_of(i).T
        vT[slot, 0:HD] = flipped[HD:128]
        old = mref[tile, 0:1]
        new = jnp.maximum(old, mnew[slot, 0:1])
        weights = jnp.exp2(sbuf[slot] - new).astype(BF16)
        factor = jnp.exp2(old - new)
        acc[tile] = acc[tile] * factor + jnp.dot(vT[slot], weights, preferred_element_type=F32)
        mref[tile, 0:1] = new

    def tiles(lo, hi):
        while lo < hi:
            end = min(lo + 2, hi)

            @pl.when(sp >= 0)
            def _():
                for i in range(lo, end):
                    if i + 1 < len(ORDER):
                        scores(i + 1)
                    weigh(i)

            lo = end

    def finish(s):
        part = acc[s // 2, :, (s % 2) * STAGE_Q : (s % 2 + 1) * STAGE_Q]
        o = (part[0:HD] / part[HD : HD + 1]).T
        for g in range(2):
            att_buf[s, :, 128 * g : 128 * g + 128] = jnp.concatenate(
                [o[2 * g * BLK : (2 * g + 1) * BLK], o[(2 * g + 1) * BLK : (2 * g + 2) * BLK]], axis=1
            ).astype(BF16)

    project(0)
    one0 = phase1(0)
    arrive(one0)
    two0 = phase2(0)
    arrive([tok_r[0]])
    tok_fr = send(toks.at[1, halves[0]], toks.at[3, halves[0]], tok_sem.at[2, 0], (sp, right))
    arrive([tok_l[1]])
    tok_fl = send(toks.at[1, halves[1]], toks.at[3, halves[1]], tok_sem.at[2, 1], (sp, left))
    project(1)
    one1 = phase1(1)
    arrive(two0)
    sib0 = share(0)
    scores(0)
    tiles(0, 1)
    arrive(one1)
    two1 = phase2(1)
    arrive([tok_r[1], tok_l[0]])
    project(2)
    one2 = phase1(2)
    arrive(sib0)
    tiles(1, 3)
    arrive([tok_fr, tok_fl])
    copies[4].wait()
    wo_half = OUT_ROWS // 4
    base = c * (OUT_ROWS // 2)
    wparts = [pl.ds(pl.multiple_of(base + k * wo_half, wo_half), wo_half) for k in (0, 1)]
    wo_r, wo_l = [None, None], [None, None]
    for i in (0, 1):
        wo_r[i] = send(wo.at[0, wparts[i]], wo.at[1, wparts[i]], wo_sem.at[0, i], (sp, right))
        wo_l[1 - i] = send(
            wo.at[0, wparts[1 - i]], wo.at[2, wparts[1 - i]], wo_sem.at[1, 1 - i], (sp, left)
        )
    project(3)
    one3 = phase1(3)
    arrive(one2)
    two2 = phase2(2)
    arrive(two1)
    sib1 = share(1)
    tiles(3, 7)
    arrive(one3)
    two3 = phase2(3)
    tiles(7, 9)
    arrive(two2)
    sib2 = share(2)
    arrive(sib1)
    tiles(9, 13)
    arrive(two3)
    sib3 = share(3)
    tiles(13, 15)
    arrive([wo_r[0]])
    wo_fr = send(wo.at[1, wparts[0]], wo.at[3, wparts[0]], wo_sem.at[2, 0], (sp, right))
    arrive([wo_l[1]])
    wo_fl = send(wo.at[2, wparts[1]], wo.at[3, wparts[1]], wo_sem.at[2, 1], (sp, left))
    arrive(sib2)
    tiles(15, 23)
    arrive([wo_r[1], wo_l[0]])
    whole = pl.ds(pl.multiple_of(base, OUT_ROWS // 2), OUT_ROWS // 2)
    wsib = [send(wo.at[k, whole], wo.at[k, whole], wsib_sem.at[k - 1], sibling) for k in (1, 2)]
    arrive(sib3)
    tiles(23, 28)
    finish(2)
    finish(3)

    def hand_over(s, half, slot, into, sem, peer):
        return send(att_buf.at[s, halves[half]], att_in.at[slot, halves[into]], att_sem.at[sem], peer)

    atts = [
        hand_over(2, 0, 0, 1, 0, (sp, left)),
        hand_over(2, 1, 1, 0, 1, (sp, right)),
        send(att_buf.at[3], att_in.at[2], att_sem.at[2], (sp, far)),
    ]
    tiles(28, 31)
    arrive([wo_fr, wo_fl])
    wsib.append(send(wo.at[3, whole], wo.at[3, whole], wsib_sem.at[2], sibling))
    tiles(31, 32)
    finish(1)
    atts.append(hand_over(1, 0, 0, 0, 3, (sp, left)))
    atts.append(hand_over(1, 1, 1, 1, 4, (sp, right)))
    finish(0)

    logs = jnp.concatenate(
        [(mref[k, 0:1] + jnp.log2(acc[k, HD : HD + 1])) * LN2 for k in (0, 1)], axis=1
    )
    tall = jnp.broadcast_to(logs, (128, NQ)).T
    places = [
        (0, tp * BLK), (HALF, tp * BLK + HALF), (0, left * BLK), (HALF, right * BLK + HALF),
        (0, left * BLK + HALF), (HALF, right * BLK), (0, far * BLK), (HALF, far * BLK + HALF),
    ]
    for k, (inner, place) in enumerate(places):
        mixed = jnp.zeros((HALF, 128), F32)
        for h in range(HEADS):
            start = (k // 2) * STAGE_Q + h * BLK + inner
            mixed = jnp.where(lane[0:HALF] == h, tall[start : start + HALF], mixed)
        lrows[pl.ds(pl.multiple_of(place, HALF), HALF)] = mixed
    log_ref[...] = lrows[...].T[0:HEADS]

    arrive(wsib)
    arrive(atts)
    pairs = [(att_buf[0], 0), (att_in[0], 2), (att_in[1], 1), (att_in[2], 3)]
    width = 512
    for n in range(D // width):
        cols = pl.ds(n * width, width)
        total = jnp.zeros((BLK, width), F32)
        for value, slot in pairs:
            total = total + jnp.dot(value, wo[slot, :, cols], preferred_element_type=F32)
        out_ref[:, cols] = total.astype(BF16)

    for copy in sends:
        copy.wait_send()


def body(tokens, query_weight, key_weight, value_weight, out_weight, query_gain, key_gain):
    any_spec = pl.BlockSpec(memory_space=pl.ANY)
    vmem = pl.BlockSpec(memory_space=pltpu.VMEM)
    dma = pltpu.SemaphoreType.DMA
    return pl.pallas_call(
        kernel,
        out_shape=(
            jax.ShapeDtypeStruct((BLK, D), BF16),
            jax.ShapeDtypeStruct((HEADS, 4 * BLK), F32),
        ),
        in_specs=[any_spec] * 5 + [vmem] * 2,
        out_specs=(vmem, vmem),
        scratch_shapes=[
            pltpu.VMEM((4, BLK, D), BF16),
            pltpu.VMEM((D, 256), BF16),
            pltpu.VMEM((128, D), BF16),
            pltpu.VMEM((4, OUT_ROWS, D), BF16),
            pltpu.VMEM((128, 128), BF16),
            pltpu.VMEM((128, 128), BF16),
            pltpu.VMEM((6, 8, 128), F32),
            pltpu.VMEM((4, HEADS, BLK, 128), BF16),
            pltpu.VMEM((NC, 16, NY, BLK, 128), BF16),
            pltpu.VMEM((2, VROWS, KC), BF16),
            pltpu.VMEM((2, KC, QT), F32),
            pltpu.VMEM((2, 8, QT), F32),
            pltpu.VMEM((2, VROWS, QT), F32),
            pltpu.VMEM((2, 8, QT), F32),
            pltpu.VMEM((4, BLK, 256), BF16),
            pltpu.VMEM((3, BLK, 256), BF16),
            pltpu.VMEM((4 * BLK, 128), F32),
            dma((5,)),
            dma((80,)),
            dma((3, 2)),
            dma((4, 2, 3)),
            dma((4, 2, 3)),
            dma((4,)),
            dma((3, 2)),
            dma((3,)),
            dma((5,)),
        ],
        compiler_params=pltpu.CompilerParams(
            collective_id=0, has_side_effects=True, vmem_limit_bytes=60 * 2**20
        ),
    )(tokens, query_weight, key_weight.T, value_weight.T, out_weight, query_gain, key_gain)


def solution(mesh):
    return jax.shard_map(
        body,
        mesh=mesh,
        in_specs=(
            P(("sp", "tp"), None),
            P(None, "tp"),
            P(None, "tp"),
            P(None, "tp"),
            P("tp", None),
            P("tp", None),
            P("tp", None),
        ),
        out_specs=(P(("sp", "tp"), None), P("tp", "sp")),
        check_vma=False,
    )
```

```python
import functools
import math

import jax
import jax.numpy as jnp
from jax import lax
from jax.experimental import pallas as pl
from jax.experimental.pallas import tpu as pltpu
from jax.sharding import PartitionSpec as P

MESH = pl.DeviceIdType.MESH
F32 = jnp.float32
BF16 = jnp.bfloat16
NZ, NY, NC, NX = 4, 4, 2, 4
BLK = 96
HALF = 48
D = 2048
HD = 64
HEADS = 4
GRID_W = 64
STAGE_Q = HEADS * BLK
NQ = 4 * STAGE_Q
KC = NY * NC * BLK
QT = 768
VROWS = 80
LOG2E = 1.4426950408889634
OUT_ROWS = 256
LN2 = 0.6931471805599453
ORDER = [(t, 0, r) for t in (0, 1) for r in range(4)]
ORDER += [(t, 1, r + d) for r in (0, 2) for t in (0, 1) for d in (0, 1)]
ORDER += [(t, 2, r + d) for r in (0, 2) for t in (1, 0) for d in (0, 1)]
ORDER += [(t, 3, r) for t in (1, 0) for r in range(4)]


def lanes(shape):
    return lax.broadcasted_iota(jnp.int32, shape, 1)


def rows(shape):
    return lax.broadcasted_iota(jnp.int32, shape, 0)


def kernel(
    tok_hbm, wq_hbm, wk_hbm, wv_hbm, wo_hbm, qg_ref, kg_ref,
    out_ref, log_ref,
    toks, wq, wkv, wo, turns, total, perm, ones, gains, q_rows, kv, vT, sbuf, mnew, acc, mref,
    att_buf, att_in, lrows, local_sem, send_sem, tok_sem, p1_sem, p2_sem, sib_sem, wo_sem, wsib_sem, att_sem,
):
    sp = lax.axis_index("sp")
    tp = lax.axis_index("tp")
    c = lax.rem(sp, 2)
    y = lax.rem(sp // 2, 4)
    z = sp // 8

    def at_zy(zz, yy):
        return ((zz * NY + yy) * NC + c, tp)

    right, left, far = lax.rem(tp + 1, 4), lax.rem(tp + 3, 4), lax.rem(tp + 2, 4)
    sibling = (sp + 1 - 2 * c, tp)
    z_peers = [at_zy(lax.rem(z + d, 4), y) for d in (1, 2, 3)]
    y_peers = [at_zy(z, lax.rem(y + d, 4)) for d in (1, 2, 3)]
    owner = [tp, left, right, far]

    copies = [
        pltpu.make_async_copy(src, dst, local_sem.at[i])
        for i, (src, dst) in enumerate(
            [
                (tok_hbm, toks.at[0]), (wk_hbm, wkv.at[pl.ds(0, HD)]), (wv_hbm, wkv.at[pl.ds(HD, HD)]),
                (wq_hbm, wq), (wo_hbm, wo.at[0]),
            ]
        )
    ]
    for copy in copies:
        copy.start()

    barrier = pltpu.get_barrier_semaphore()
    peers = [(sp, right), (sp, left), (sp, far), sibling] + z_peers + y_peers
    for peer in peers:
        pl.semaphore_signal(barrier, inc=1, device_id=peer, device_id_type=MESH)

    sends = []

    def send(src, dst, recv, peer):
        copy = pltpu.make_async_remote_copy(
            src_ref=src, dst_ref=dst, send_sem=send_sem.at[len(sends)], recv_sem=recv,
            device_id=peer, device_id_type=MESH,
        )
        sends.append(copy)
        copy.start()
        return copy

    i2, j2 = rows((128, 128)), lanes((128, 128))
    lower = (j2 & 31) < 16
    perm[...] = jnp.where(
        lower & (i2 == j2 + 16), -1.0, jnp.where((~lower) & (i2 == j2 - 16), 1.0, 0.0)
    ).astype(BF16)
    ones[...] = jnp.where((i2 // 64) == (j2 // 64), 1.0 / 64.0, 0.0).astype(BF16)
    qg = qg_ref[...].astype(F32)
    kg = kg_ref[...].astype(F32)
    lane1 = lanes((8, 128))
    for g in range(3):
        if g < 2:
            pair = jnp.concatenate([qg[2 * g : 2 * g + 1], qg[2 * g + 1 : 2 * g + 2]], axis=1)
            pair = pair * (HD ** (-0.5) * LOG2E)
        else:
            pair = jnp.concatenate([kg, kg], axis=1)
        pair = jnp.broadcast_to(pair, (8, 128))
        gains[2 * g] = pair
        gains[2 * g + 1] = jnp.where((lane1 & 31) < 16, pltpu.roll(pair, 112, 1), pltpu.roll(pair, 16, 1))

    lane = lanes((BLK, 128))
    inside = lane & 63
    exponent = (inside & 15).astype(F32) * (-math.log(10000.0) / 16.0)
    freq = jnp.exp(exponent)

    for s in range(4):
        within = rows((BLK, 128))
        if s == 1:
            place = jnp.where(within < HALF, left * BLK, right * BLK) + within
        elif s == 2:
            place = jnp.where(within < HALF, left * BLK + HALF, right * BLK - HALF) + within
        else:
            place = owner[s] * BLK + within
        place = sp * 384 + place
        grid_row = (place >> 6).astype(F32)
        grid_col = (place & 63).astype(F32)
        angle = jnp.where(inside < 32, grid_row, grid_col) * freq
        turns[0, s], turns[1, s] = jnp.cos(angle), jnp.sin(angle)

    pl.semaphore_wait(barrier, len(peers))
    copies[0].wait()
    halves = (pl.ds(0, HALF), pl.ds(HALF, HALF))
    tok_r, tok_l = [None, None], [None, None]
    for i in (0, 1):
        tok_r[i] = send(toks.at[0, halves[i]], toks.at[1 + i, halves[0]], tok_sem.at[0, i], (sp, right))
        tok_l[1 - i] = send(
            toks.at[0, halves[1 - i]], toks.at[1 + i, halves[1]], tok_sem.at[1, 1 - i], (sp, left)
        )
    for copy in copies[1:4]:
        copy.wait()

    def prepare(s, raw, g):
        value = raw.astype(F32)
        turned = jnp.dot(raw, perm[...], preferred_element_type=F32)
        square = value * value
        high = square.astype(BF16)
        low = (square - high.astype(F32)).astype(BF16)
        mean = jnp.dot(high, ones[...], preferred_element_type=F32) + jnp.dot(
            low, ones[...], preferred_element_type=F32
        )
        inverse = lax.rsqrt(mean + 1e-6)
        return inverse * (
            value * gains[2 * g, 0:1] * turns[0, s] + turned * gains[2 * g + 1, 0:1] * turns[1, s]
        )

    def project_keys(s):
        raw = lax.dot_general(
            toks[s], wkv[...], (((1,), (1,)), ((), ())), preferred_element_type=F32
        ).astype(BF16)
        slab = jnp.where(lane < 64, prepare(s, raw, 2), raw.astype(F32))
        kv[c, 4 * s + z, y] = slab.astype(BF16)

    def project_queries(s):
        raw = jnp.dot(toks[s], wq[...], preferred_element_type=F32).astype(BF16)
        for g in range(2):
            done = prepare(s, raw[:, 128 * g : 128 * g + 128], g)
            q_rows[s, 2 * g] = jnp.where(lane < 64, done, 0.0).astype(BF16)
            q_rows[s, 2 * g + 1] = jnp.where(lane < 64, pltpu.roll(done, 64, 1), 0.0).astype(BF16)

    def phase1(s):
        a = kv.at[c, 4 * s + z, y, halves[0]]
        b = kv.at[c, 4 * s + z, y, halves[1]]
        first = [send(a, a, p1_sem.at[s, 0, d], z_peers[d]) for d in range(3)]
        return first + [send(b, b, p1_sem.at[s, 1, d], y_peers[d]) for d in range(3)]

    def phase2(s):
        a = kv.at[c, pl.ds(4 * s, 4), y, halves[0]]
        b = kv.at[c, 4 * s + z, :, halves[1]]
        first = [send(a, a, p2_sem.at[s, 0, d], y_peers[d]) for d in range(3)]
        return first + [send(b, b, p2_sem.at[s, 1, d], z_peers[d]) for d in range(3)]

    def share(s):
        a = kv.at[c, pl.ds(4 * s, 4)]
        return [send(a, a, sib_sem.at[s], sibling)]

    def arrive(group):
        for copy in group:
            copy.wait_recv()

    acc[...] = jnp.zeros_like(acc)
    mref[...] = jnp.full_like(mref, -1e30)
    vT[:, HD:VROWS] = jnp.ones((2, VROWS - HD, KC), BF16)
    per_tile = QT // STAGE_Q

    def keys_of(i):
        s, r = ORDER[i][1:]
        core = lax.rem(c + r // 2, 2)
        place = 4 * s + 2 * (r % 2)
        return kv[core, place : place + 2].reshape(KC, 128)

    def scores(i):
        tile, slot = ORDER[i][0], i % 2
        q = q_rows[tile * per_tile : (tile + 1) * per_tile].reshape(QT, 128)
        s = lax.dot_general(keys_of(i), q, (((1,), (1,)), ((), ())), preferred_element_type=F32)
        sbuf[slot] = s
        mnew[slot, 0:1] = jnp.max(s, axis=0, keepdims=True)

    def weigh(i):
        tile, slot = ORDER[i][0], i % 2
        flipped = keys_of(i).T
        vT[slot, 0:HD] = flipped[HD:128]
        old = mref[tile, 0:1]
        new = jnp.maximum(old, mnew[slot, 0:1])
        weights = jnp.exp2(sbuf[slot] - new).astype(BF16)
        factor = jnp.exp2(old - new)
        acc[tile] = acc[tile] * factor + jnp.dot(vT[slot], weights, preferred_element_type=F32)
        mref[tile, 0:1] = new

    def tiles(lo, hi):
        while lo < hi:
            end = min(lo + 2, hi)

            @pl.when(sp >= 0)
            def _():
                for i in range(lo, end):
                    if i + 1 < len(ORDER):
                        scores(i + 1)
                    weigh(i)

            lo = end

    def finish(s):
        part = acc[s // 2, :, (s % 2) * STAGE_Q : (s % 2 + 1) * STAGE_Q]
        o = (part[0:HD] / part[HD : HD + 1]).T
        for g in range(2):
            att_buf[s, :, 128 * g : 128 * g + 128] = jnp.concatenate(
                [o[2 * g * BLK : (2 * g + 1) * BLK], o[(2 * g + 1) * BLK : (2 * g + 2) * BLK]], axis=1
            ).astype(BF16)

    project_keys(0)
    one0 = phase1(0)
    project_queries(0)
    arrive(one0)
    two0 = phase2(0)
    arrive([tok_r[0]])
    tok_fr = send(toks.at[1, halves[0]], toks.at[3, halves[0]], tok_sem.at[2, 0], (sp, right))
    arrive([tok_l[1]])
    tok_fl = send(toks.at[1, halves[1]], toks.at[3, halves[1]], tok_sem.at[2, 1], (sp, left))
    project_keys(1)
    one1 = phase1(1)
    project_queries(1)
    arrive(two0)
    sib0 = share(0)
    scores(0)
    tiles(0, 1)
    arrive(one1)
    two1 = phase2(1)
    arrive([tok_r[1], tok_l[0]])
    project_keys(2)
    one2 = phase1(2)
    project_queries(2)
    arrive(sib0)
    tiles(1, 3)
    arrive([tok_fr, tok_fl])
    copies[4].wait()
    wo_half = OUT_ROWS // 4
    base = c * (OUT_ROWS // 2)
    wparts = [pl.ds(pl.multiple_of(base + k * wo_half, wo_half), wo_half) for k in (0, 1)]
    wo_r, wo_l = [None, None], [None, None]
    for i in (0, 1):
        wo_r[i] = send(wo.at[0, wparts[i]], wo.at[1, wparts[i]], wo_sem.at[0, i], (sp, right))
        wo_l[1 - i] = send(
            wo.at[0, wparts[1 - i]], wo.at[2, wparts[1 - i]], wo_sem.at[1, 1 - i], (sp, left)
        )
    project_keys(3)
    one3 = phase1(3)
    project_queries(3)
    tiles(3, 5)
    arrive(one2)
    two2 = phase2(2)
    arrive(two1)
    sib1 = share(1)
    tiles(5, 7)
    arrive(one3)
    two3 = phase2(3)
    tiles(7, 11)
    arrive(sib1)
    tiles(11, 13)
    arrive(two2)
    sib2 = share(2)
    tiles(13, 17)
    arrive([wo_r[0]])
    wo_fr = send(wo.at[1, wparts[0]], wo.at[3, wparts[0]], wo_sem.at[2, 0], (sp, right))
    arrive([wo_l[1]])
    wo_fl = send(wo.at[2, wparts[1]], wo.at[3, wparts[1]], wo_sem.at[2, 1], (sp, left))
    arrive(two3)
    sib3 = share(3)
    tiles(17, 19)
    arrive(sib2)
    tiles(19, 23)
    arrive([wo_r[1], wo_l[0]])
    whole = pl.ds(pl.multiple_of(base, OUT_ROWS // 2), OUT_ROWS // 2)
    wsib = [send(wo.at[k, whole], wo.at[k, whole], wsib_sem.at[k - 1], sibling) for k in (1, 2)]
    tiles(23, 25)
    arrive(sib3)
    tiles(25, 28)
    finish(2)
    finish(3)

    def hand_over(s, half, slot, into, sem, peer):
        return send(att_buf.at[s, halves[half]], att_in.at[slot, halves[into]], att_sem.at[sem], peer)

    atts = [
        hand_over(2, 0, 0, 1, 0, (sp, left)),
        hand_over(2, 1, 1, 0, 1, (sp, right)),
        send(att_buf.at[3], att_in.at[2], att_sem.at[2], (sp, far)),
    ]
    tiles(28, 29)
    arrive([wo_fr, wo_fl])
    wsib.append(send(wo.at[3, whole], wo.at[3, whole], wsib_sem.at[2], sibling))
    tiles(29, 32)
    finish(1)
    atts.append(hand_over(1, 0, 0, 0, 3, (sp, left)))
    atts.append(hand_over(1, 1, 1, 1, 4, (sp, right)))
    finish(0)

    logs = jnp.concatenate(
        [(mref[k, 0:1] + jnp.log2(acc[k, HD : HD + 1])) * LN2 for k in (0, 1)], axis=1
    )
    tall = jnp.broadcast_to(logs, (128, NQ)).T
    places = [
        (0, tp * BLK), (HALF, tp * BLK + HALF), (0, left * BLK), (HALF, right * BLK + HALF),
        (0, left * BLK + HALF), (HALF, right * BLK), (0, far * BLK), (HALF, far * BLK + HALF),
    ]
    for k, (inner, place) in enumerate(places):
        mixed = jnp.zeros((HALF, 128), F32)
        for h in range(HEADS):
            start = (k // 2) * STAGE_Q + h * BLK + inner
            mixed = jnp.where(lane[0:HALF] == h, tall[start : start + HALF], mixed)
        lrows[pl.ds(pl.multiple_of(place, HALF), HALF)] = mixed
    log_ref[...] = lrows[...].T[0:HEADS]

    width = 512

    def out_product(value, slot, part, first=False, last=False):
        for n in range(D // width):
            cols = pl.ds(n * width, width)
            product = jnp.dot(value, wo[slot, :, cols], preferred_element_type=F32)
            if not first:
                product = product + total[part, cols]
            if last:
                out_ref[part, cols] = product.astype(BF16)
            else:
                total[part, cols] = product

    out_product(att_buf[0], 0, pl.ds(0, BLK), first=True)
    arrive(wsib[0:2])
    arrive(atts[0:2])
    out_product(att_in[1, halves[0]], 1, halves[0])
    out_product(att_in[0, halves[1]], 2, halves[1])
    arrive(wsib[2:3])
    arrive(atts[2:3])
    out_product(att_in[2], 3, pl.ds(0, BLK))
    arrive(atts[3:5])
    out_product(att_in[0, halves[0]], 2, halves[0], last=True)
    out_product(att_in[1, halves[1]], 1, halves[1], last=True)

    for copy in sends:
        copy.wait_send()


def body(tokens, query_weight, key_weight, value_weight, out_weight, query_gain, key_gain):
    any_spec = pl.BlockSpec(memory_space=pl.ANY)
    vmem = pl.BlockSpec(memory_space=pltpu.VMEM)
    dma = pltpu.SemaphoreType.DMA
    return pl.pallas_call(
        kernel,
        out_shape=(
            jax.ShapeDtypeStruct((BLK, D), BF16),
            jax.ShapeDtypeStruct((HEADS, 4 * BLK), F32),
        ),
        in_specs=[any_spec] * 5 + [vmem] * 2,
        out_specs=(vmem, vmem),
        scratch_shapes=[
            pltpu.VMEM((4, BLK, D), BF16),
            pltpu.VMEM((D, 256), BF16),
            pltpu.VMEM((128, D), BF16),
            pltpu.VMEM((4, OUT_ROWS, D), BF16),
            pltpu.VMEM((2, 4, BLK, 128), F32),
            pltpu.VMEM((BLK, D), F32),
            pltpu.VMEM((128, 128), BF16),
            pltpu.VMEM((128, 128), BF16),
            pltpu.VMEM((6, 8, 128), F32),
            pltpu.VMEM((4, HEADS, BLK, 128), BF16),
            pltpu.VMEM((NC, 16, NY, BLK, 128), BF16),
            pltpu.VMEM((2, VROWS, KC), BF16),
            pltpu.VMEM((2, KC, QT), F32),
            pltpu.VMEM((2, 8, QT), F32),
            pltpu.VMEM((2, VROWS, QT), F32),
            pltpu.VMEM((2, 8, QT), F32),
            pltpu.VMEM((4, BLK, 256), BF16),
            pltpu.VMEM((3, BLK, 256), BF16),
            pltpu.VMEM((4 * BLK, 128), F32),
            dma((5,)),
            dma((80,)),
            dma((3, 2)),
            dma((4, 2, 3)),
            dma((4, 2, 3)),
            dma((4,)),
            dma((3, 2)),
            dma((3,)),
            dma((5,)),
        ],
        compiler_params=pltpu.CompilerParams(
            collective_id=0, has_side_effects=True, vmem_limit_bytes=60 * 2**20
        ),
    )(tokens, query_weight, key_weight.T, value_weight.T, out_weight, query_gain, key_gain)


def solution(mesh):
    return jax.shard_map(
        body,
        mesh=mesh,
        in_specs=(
            P(("sp", "tp"), None),
            P(None, "tp"),
            P(None, "tp"),
            P(None, "tp"),
            P("tp", None),
            P("tp", None),
            P("tp", None),
        ),
        out_specs=(P(("sp", "tp"), None), P("tp", "sp")),
        check_vma=False,
    )
```

```python
import functools
import math

import jax
import jax.numpy as jnp
from jax import lax
from jax.experimental import pallas as pl
from jax.experimental.pallas import tpu as pltpu
from jax.sharding import PartitionSpec as P

MESH = pl.DeviceIdType.MESH
F32 = jnp.float32
BF16 = jnp.bfloat16
NZ, NY, NC, NX = 4, 4, 2, 4
BLK = 96
HALF = 48
D = 2048
HD = 64
HEADS = 4
GRID_W = 64
STAGE_Q = HEADS * BLK
NQ = 4 * STAGE_Q
KC = NY * NC * BLK
QT = 768
VROWS = 80
LOG2E = 1.4426950408889634
OUT_ROWS = 256
LN2 = 0.6931471805599453
ORDER = [(t, 0, r) for t in (0, 1) for r in range(4)]
ORDER += [(t, 1, r + d) for r in (0, 2) for t in (0, 1) for d in (0, 1)]
ORDER += [(t, 2, r + d) for r in (0, 2) for t in (1, 0) for d in (0, 1)]
ORDER += [(t, 3, r) for t in (1, 0) for r in range(4)]


def lanes(shape):
    return lax.broadcasted_iota(jnp.int32, shape, 1)


def rows(shape):
    return lax.broadcasted_iota(jnp.int32, shape, 0)


def kernel(
    tok_hbm, wq_hbm, wk_hbm, wv_hbm, wo_hbm, qg_ref, kg_ref,
    out_hbm, log_hbm,
    toks, wq, wkv, wo, turns, total, perm, ones, gains, q_rows, kv, vT, sbuf, mnew, acc, mref,
    out_ref, log_ref, att_buf, att_in, lrows, local_sem, send_sem, tok_sem, p1_sem, p2_sem, sib_sem, wo_sem, wsib_sem, att_sem,
):
    sp = lax.axis_index("sp")
    tp = lax.axis_index("tp")
    c = lax.rem(sp, 2)
    y = lax.rem(sp // 2, 4)
    z = sp // 8

    def at_zy(zz, yy):
        return ((zz * NY + yy) * NC + c, tp)

    right, left, far = lax.rem(tp + 1, 4), lax.rem(tp + 3, 4), lax.rem(tp + 2, 4)
    sibling = (sp + 1 - 2 * c, tp)
    z_peers = [at_zy(lax.rem(z + d, 4), y) for d in (1, 2, 3)]
    y_peers = [at_zy(z, lax.rem(y + d, 4)) for d in (1, 2, 3)]
    owner = [tp, left, right, far]

    copies = [
        pltpu.make_async_copy(src, dst, local_sem.at[i])
        for i, (src, dst) in enumerate(
            [
                (tok_hbm, toks.at[0]), (wk_hbm, wkv.at[pl.ds(0, HD)]), (wv_hbm, wkv.at[pl.ds(HD, HD)]),
                (wq_hbm, wq), (wo_hbm, wo.at[0]),
            ]
        )
    ]
    for copy in copies:
        copy.start()

    barrier = pltpu.get_barrier_semaphore()
    peers = [(sp, right), (sp, left), (sp, far), sibling] + z_peers + y_peers
    for peer in peers:
        pl.semaphore_signal(barrier, inc=1, device_id=peer, device_id_type=MESH)

    sends = []

    def send(src, dst, recv, peer):
        copy = pltpu.make_async_remote_copy(
            src_ref=src, dst_ref=dst, send_sem=send_sem.at[len(sends)], recv_sem=recv,
            device_id=peer, device_id_type=MESH,
        )
        sends.append(copy)
        copy.start()
        return copy

    i2, j2 = rows((128, 128)), lanes((128, 128))
    lower = (j2 & 31) < 16
    perm[...] = jnp.where(
        lower & (i2 == j2 + 16), -1.0, jnp.where((~lower) & (i2 == j2 - 16), 1.0, 0.0)
    ).astype(BF16)
    ones[...] = jnp.where((i2 // 64) == (j2 // 64), 1.0 / 64.0, 0.0).astype(BF16)
    qg = qg_ref[...].astype(F32)
    kg = kg_ref[...].astype(F32)
    lane1 = lanes((8, 128))
    for g in range(3):
        if g < 2:
            pair = jnp.concatenate([qg[2 * g : 2 * g + 1], qg[2 * g + 1 : 2 * g + 2]], axis=1)
            pair = pair * (HD ** (-0.5) * LOG2E)
        else:
            pair = jnp.concatenate([kg, kg], axis=1)
        pair = jnp.broadcast_to(pair, (8, 128))
        gains[2 * g] = pair
        gains[2 * g + 1] = jnp.where((lane1 & 31) < 16, pltpu.roll(pair, 112, 1), pltpu.roll(pair, 16, 1))

    lane = lanes((BLK, 128))
    inside = lane & 63
    exponent = (inside & 15).astype(F32) * (-math.log(10000.0) / 16.0)
    freq = jnp.exp(exponent)

    for s in range(4):
        within = rows((BLK, 128))
        if s == 1:
            place = jnp.where(within < HALF, left * BLK, right * BLK) + within
        elif s == 2:
            place = jnp.where(within < HALF, left * BLK + HALF, right * BLK - HALF) + within
        else:
            place = owner[s] * BLK + within
        place = sp * 384 + place
        grid_row = (place >> 6).astype(F32)
        grid_col = (place & 63).astype(F32)
        angle = jnp.where(inside < 32, grid_row, grid_col) * freq
        turns[0, s], turns[1, s] = jnp.cos(angle), jnp.sin(angle)

    vT[:, HD:VROWS] = jnp.ones((16, VROWS - HD, KC), BF16)
    pl.semaphore_wait(barrier, len(peers))
    copies[0].wait()
    halves = (pl.ds(0, HALF), pl.ds(HALF, HALF))
    tok_r, tok_l = [None, None], [None, None]
    for i in (0, 1):
        tok_r[i] = send(toks.at[0, halves[i]], toks.at[1 + i, halves[0]], tok_sem.at[0, i], (sp, right))
        tok_l[1 - i] = send(
            toks.at[0, halves[1 - i]], toks.at[1 + i, halves[1]], tok_sem.at[1, 1 - i], (sp, left)
        )
    for copy in copies[1:4]:
        copy.wait()

    def prepare(s, raw, g):
        value = raw.astype(F32)
        turned = jnp.dot(raw, perm[...], preferred_element_type=F32)
        square = value * value
        high = square.astype(BF16)
        low = (square - high.astype(F32)).astype(BF16)
        mean = jnp.dot(high, ones[...], preferred_element_type=F32) + jnp.dot(
            low, ones[...], preferred_element_type=F32
        )
        inverse = lax.rsqrt(mean + 1e-6)
        return inverse * (
            value * gains[2 * g, 0:1] * turns[0, s] + turned * gains[2 * g + 1, 0:1] * turns[1, s]
        )

    def project_keys(s):
        raw = lax.dot_general(
            toks[s], wkv[...], (((1,), (1,)), ((), ())), preferred_element_type=F32
        ).astype(BF16)
        slab = jnp.where(lane < 64, prepare(s, raw, 2), raw.astype(F32))
        kv[c, 4 * s + z, y] = slab.astype(BF16)

    def project_queries(s):
        raw = jnp.dot(toks[s], wq[...], preferred_element_type=F32).astype(BF16)
        for g in range(2):
            done = prepare(s, raw[:, 128 * g : 128 * g + 128], g)
            q_rows[s, 2 * g] = jnp.where(lane < 64, done, 0.0).astype(BF16)
            q_rows[s, 2 * g + 1] = jnp.where(lane < 64, pltpu.roll(done, 64, 1), 0.0).astype(BF16)

    def phase1(s):
        a = kv.at[c, 4 * s + z, y, halves[0]]
        b = kv.at[c, 4 * s + z, y, halves[1]]
        first = [send(a, a, p1_sem.at[s, 0, d], z_peers[d]) for d in range(3)]
        return first + [send(b, b, p1_sem.at[s, 1, d], y_peers[d]) for d in range(3)]

    def phase2(s):
        a = kv.at[c, pl.ds(4 * s, 4), y, halves[0]]
        b = kv.at[c, 4 * s + z, :, halves[1]]
        first = [send(a, a, p2_sem.at[s, 0, d], y_peers[d]) for d in range(3)]
        return first + [send(b, b, p2_sem.at[s, 1, d], z_peers[d]) for d in range(3)]

    def share(s):
        a = kv.at[c, pl.ds(4 * s, 4)]
        return [send(a, a, sib_sem.at[s], sibling)]

    def arrive(group):
        for copy in group:
            copy.wait_recv()

    acc[...] = jnp.zeros_like(acc)
    mref[...] = jnp.full_like(mref, -1e30)
    per_tile = QT // STAGE_Q

    def keys_of(i):
        s, r = ORDER[i][1:]
        core = lax.rem(c + r // 2, 2)
        place = 4 * s + 2 * (r % 2)
        return kv[core, place : place + 2].reshape(KC, 128)

    def scores(i, part):
        tile, slot = ORDER[i][0], i % 2
        q = q_rows[tile * per_tile : (tile + 1) * per_tile].reshape(QT, 128)[part]
        s = lax.dot_general(keys_of(i), q, (((1,), (1,)), ((), ())), preferred_element_type=F32)
        sbuf[slot, :, part] = s
        mnew[slot, 0:1, part] = jnp.max(s, axis=0, keepdims=True)

    def weigh(i, part):
        tile, slot = ORDER[i][0], i % 2
        chunk = 4 * ORDER[i][1] + ORDER[i][2]
        if part.start == 0 and ORDER[i][1:] not in [other[1:] for other in ORDER[:i]]:
            flipped = keys_of(i).T
            vT[chunk, 0:HD] = flipped[HD:128]
        for cols in [part]:
            old = mref[tile, 0:1, cols]
            new = jnp.maximum(old, mnew[slot, 0:1, cols])
            weights = jnp.exp2(sbuf[slot, :, cols] - new).astype(BF16)
            factor = jnp.exp2(old - new)
            acc[tile, :, cols] = acc[tile, :, cols] * factor + jnp.dot(
                vT[chunk], weights, preferred_element_type=F32
            )
            mref[tile, 0:1, cols] = new

    def tiles(lo, hi, parts=(0, 1)):
        while lo < hi:
            end = min(lo + 2, hi)

            @pl.when(sp >= 0)
            def _():
                for i in range(lo, end):
                    for j in parts:
                        cols = slice(j * STAGE_Q, (j + 1) * STAGE_Q)
                        if i + 1 < len(ORDER):
                            scores(i + 1, cols)
                        weigh(i, cols)

            lo = end

    def finish(s):
        part = acc[s // 2, :, (s % 2) * STAGE_Q : (s % 2 + 1) * STAGE_Q]
        o = (part[0:HD] / part[HD : HD + 1]).T
        for g in range(2):
            att_buf[s, :, 128 * g : 128 * g + 128] = jnp.concatenate(
                [o[2 * g * BLK : (2 * g + 1) * BLK], o[(2 * g + 1) * BLK : (2 * g + 2) * BLK]], axis=1
            ).astype(BF16)

    project_keys(0)
    one0 = phase1(0)
    project_queries(0)
    arrive(one0)
    two0 = phase2(0)
    arrive([tok_r[0]])
    tok_fr = send(toks.at[1, halves[0]], toks.at[3, halves[0]], tok_sem.at[2, 0], (sp, right))
    arrive([tok_l[1]])
    tok_fl = send(toks.at[1, halves[1]], toks.at[3, halves[1]], tok_sem.at[2, 1], (sp, left))
    project_keys(1)
    one1 = phase1(1)
    project_queries(1)
    arrive(two0)
    sib0 = share(0)
    scores(0, slice(0, QT))
    tiles(0, 1)
    arrive(one1)
    two1 = phase2(1)
    arrive([tok_r[1], tok_l[0]])
    project_keys(2)
    one2 = phase1(2)
    project_queries(2)
    arrive(sib0)
    tiles(1, 3)
    arrive([tok_fr, tok_fl])
    copies[4].wait()
    wo_half = OUT_ROWS // 4
    base = c * (OUT_ROWS // 2)
    wparts = [pl.ds(pl.multiple_of(base + k * wo_half, wo_half), wo_half) for k in (0, 1)]
    wo_r, wo_l = [None, None], [None, None]
    for i in (0, 1):
        wo_r[i] = send(wo.at[0, wparts[i]], wo.at[1, wparts[i]], wo_sem.at[0, i], (sp, right))
        wo_l[1 - i] = send(
            wo.at[0, wparts[1 - i]], wo.at[2, wparts[1 - i]], wo_sem.at[1, 1 - i], (sp, left)
        )
    project_keys(3)
    one3 = phase1(3)
    project_queries(3)
    tiles(3, 5)
    arrive(one2)
    two2 = phase2(2)
    arrive(two1)
    sib1 = share(1)
    tiles(5, 7)
    arrive(one3)
    two3 = phase2(3)
    tiles(7, 11)
    arrive(sib1)
    tiles(11, 13)
    arrive(two2)
    sib2 = share(2)
    tiles(13, 17)
    arrive([wo_r[0]])
    wo_fr = send(wo.at[1, wparts[0]], wo.at[3, wparts[0]], wo_sem.at[2, 0], (sp, right))
    arrive([wo_l[1]])
    wo_fl = send(wo.at[2, wparts[1]], wo.at[3, wparts[1]], wo_sem.at[2, 1], (sp, left))
    arrive(two3)
    sib3 = share(3)
    tiles(17, 19)
    arrive(sib2)
    tiles(19, 23)
    arrive([wo_r[1], wo_l[0]])
    whole = pl.ds(pl.multiple_of(base, OUT_ROWS // 2), OUT_ROWS // 2)
    wsib = [send(wo.at[k, whole], wo.at[k, whole], wsib_sem.at[k - 1], sibling) for k in (1, 2)]
    tiles(23, 25)
    arrive(sib3)
    tiles(25, 28)
    finish(2)
    finish(3)

    def hand_over(s, half, slot, into, sem, peer):
        return send(att_buf.at[s, halves[half]], att_in.at[slot, halves[into]], att_sem.at[sem], peer)

    atts = [
        hand_over(2, 0, 0, 1, 0, (sp, left)),
        hand_over(2, 1, 1, 0, 1, (sp, right)),
        send(att_buf.at[3], att_in.at[2], att_sem.at[2], (sp, far)),
    ]
    tiles(28, 32, (1,))
    finish(1)
    atts.append(hand_over(1, 0, 0, 0, 3, (sp, left)))
    atts.append(hand_over(1, 1, 1, 1, 4, (sp, right)))
    arrive([wo_fr, wo_fl])
    wsib.append(send(wo.at[3, whole], wo.at[3, whole], wsib_sem.at[2], sibling))
    tiles(28, 32, (0,))
    finish(0)

    logs = jnp.concatenate(
        [(mref[k, 0:1] + jnp.log2(acc[k, HD : HD + 1])) * LN2 for k in (0, 1)], axis=1
    )
    tall = jnp.broadcast_to(logs, (128, NQ)).T
    places = [
        (0, tp * BLK), (HALF, tp * BLK + HALF), (0, left * BLK), (HALF, right * BLK + HALF),
        (0, left * BLK + HALF), (HALF, right * BLK), (0, far * BLK), (HALF, far * BLK + HALF),
    ]
    for k, (inner, place) in enumerate(places):
        mixed = jnp.zeros((HALF, 128), F32)
        for h in range(HEADS):
            start = (k // 2) * STAGE_Q + h * BLK + inner
            mixed = jnp.where(lane[0:HALF] == h, tall[start : start + HALF], mixed)
        lrows[pl.ds(pl.multiple_of(place, HALF), HALF)] = mixed
    log_ref[...] = lrows[...].T[0:HEADS]
    leaving = [pltpu.make_async_copy(log_ref, log_hbm, local_sem.at[5])]
    leaving[0].start()

    width = 512

    def out_product(value, slot, part, first=False, last=False):
        for n in range(D // width):
            cols = pl.ds(n * width, width)
            product = jnp.dot(value, wo[slot, :, cols], preferred_element_type=F32)
            if not first:
                product = product + total[part, cols]
            if last:
                out_ref[part, cols] = product.astype(BF16)
                leaving.append(
                    pltpu.make_async_copy(
                        out_ref.at[part, cols], out_hbm.at[part, cols], local_sem.at[5 + len(leaving)]
                    )
                )
                leaving[-1].start()
            else:
                total[part, cols] = product

    out_product(att_buf[0], 0, pl.ds(0, BLK), first=True)
    arrive(wsib[0:2])
    arrive(atts[0:2])
    out_product(att_in[1, halves[0]], 1, halves[0])
    out_product(att_in[0, halves[1]], 2, halves[1])
    arrive(wsib[2:3])
    arrive(atts[2:3])
    out_product(att_in[2], 3, pl.ds(0, BLK))
    arrive(atts[3:5])
    out_product(att_in[0, halves[0]], 2, halves[0], last=True)
    out_product(att_in[1, halves[1]], 1, halves[1], last=True)

    for copy in leaving:
        copy.wait()
    for copy in sends:
        copy.wait_send()


def body(tokens, query_weight, key_weight, value_weight, out_weight, query_gain, key_gain):
    any_spec = pl.BlockSpec(memory_space=pl.ANY)
    vmem = pl.BlockSpec(memory_space=pltpu.VMEM)
    dma = pltpu.SemaphoreType.DMA
    return pl.pallas_call(
        kernel,
        out_shape=(
            jax.ShapeDtypeStruct((BLK, D), BF16),
            jax.ShapeDtypeStruct((HEADS, 4 * BLK), F32),
        ),
        in_specs=[any_spec] * 5 + [vmem] * 2,
        out_specs=(any_spec, any_spec),
        scratch_shapes=[
            pltpu.VMEM((4, BLK, D), BF16),
            pltpu.VMEM((D, 256), BF16),
            pltpu.VMEM((128, D), BF16),
            pltpu.VMEM((4, OUT_ROWS, D), BF16),
            pltpu.VMEM((2, 4, BLK, 128), F32),
            pltpu.VMEM((BLK, D), F32),
            pltpu.VMEM((128, 128), BF16),
            pltpu.VMEM((128, 128), BF16),
            pltpu.VMEM((6, 8, 128), F32),
            pltpu.VMEM((4, HEADS, BLK, 128), BF16),
            pltpu.VMEM((NC, 16, NY, BLK, 128), BF16),
            pltpu.VMEM((16, VROWS, KC), BF16),
            pltpu.VMEM((2, KC, QT), F32),
            pltpu.VMEM((2, 8, QT), F32),
            pltpu.VMEM((2, VROWS, QT), F32),
            pltpu.VMEM((2, 8, QT), F32),
            pltpu.VMEM((BLK, D), BF16),
            pltpu.VMEM((HEADS, 4 * BLK), F32),
            pltpu.VMEM((4, BLK, 256), BF16),
            pltpu.VMEM((3, BLK, 256), BF16),
            pltpu.VMEM((4 * BLK, 128), F32),
            dma((14,)),
            dma((80,)),
            dma((3, 2)),
            dma((4, 2, 3)),
            dma((4, 2, 3)),
            dma((4,)),
            dma((3, 2)),
            dma((3,)),
            dma((5,)),
        ],
        compiler_params=pltpu.CompilerParams(
            collective_id=0, has_side_effects=True, vmem_limit_bytes=60 * 2**20
        ),
    )(tokens, query_weight, key_weight.T, value_weight.T, out_weight, query_gain, key_gain)


def solution(mesh):
    return jax.shard_map(
        body,
        mesh=mesh,
        in_specs=(
            P(("sp", "tp"), None),
            P(None, "tp"),
            P(None, "tp"),
            P(None, "tp"),
            P("tp", None),
            P("tp", None),
            P("tp", None),
        ),
        out_specs=(P(("sp", "tp"), None), P("tp", "sp")),
        check_vma=False,
    )
```

```python
import functools
import math

import jax
import jax.numpy as jnp
from jax import lax
from jax.experimental import pallas as pl
from jax.experimental.pallas import tpu as pltpu
from jax.sharding import PartitionSpec as P

MESH = pl.DeviceIdType.MESH
F32 = jnp.float32
BF16 = jnp.bfloat16
NZ, NY, NC, NX = 4, 4, 2, 4
BLK = 96
HALF = 48
D = 2048
HD = 64
HEADS = 4
GRID_W = 64
STAGE_Q = HEADS * BLK
NQ = 4 * STAGE_Q
KC = NY * NC * BLK
QT = 768
VROWS = 80
LOG2E = 1.4426950408889634
OUT_ROWS = 256
LN2 = 0.6931471805599453
ORDER = [(t, 0, r) for t in (0, 1) for r in range(4)]
ORDER += [(t, 1, r + d) for r in (0, 2) for t in (0, 1) for d in (0, 1)]
ORDER += [(t, 2, r + d) for r in (0, 2) for t in (1, 0) for d in (0, 1)]
ORDER += [(t, 3, r) for t in (1, 0) for r in range(4)]


def lanes(shape):
    return lax.broadcasted_iota(jnp.int32, shape, 1)


def rows(shape):
    return lax.broadcasted_iota(jnp.int32, shape, 0)


def kernel(
    tok_hbm, wq_hbm, wk_hbm, wv_hbm, wo_hbm, qg_ref, kg_ref,
    out_hbm, log_hbm,
    toks, wq, wkv, wo, turns, total, perm, ones, gains, q_rows, kv, vT, sbuf, mnew, acc, mref,
    out_ref, log_ref, att_buf, att_in, lrows, local_sem, send_sem, tok_sem, p1_sem, p2_sem, sib_sem, wo_sem, wsib_sem, att_sem,
):
    sp = lax.axis_index("sp")
    tp = lax.axis_index("tp")
    c = lax.rem(sp, 2)
    y = lax.rem(sp // 2, 4)
    z = sp // 8

    def at_zy(zz, yy):
        return ((zz * NY + yy) * NC + c, tp)

    right, left, far = lax.rem(tp + 1, 4), lax.rem(tp + 3, 4), lax.rem(tp + 2, 4)
    sibling = (sp + 1 - 2 * c, tp)
    z_peers = [at_zy(lax.rem(z + d, 4), y) for d in (1, 2, 3)]
    y_peers = [at_zy(z, lax.rem(y + d, 4)) for d in (1, 2, 3)]
    owner = [tp, left, right, far]

    copies = [
        pltpu.make_async_copy(src, dst, local_sem.at[i])
        for i, (src, dst) in enumerate(
            [
                (tok_hbm, toks.at[0]), (wk_hbm, wkv.at[pl.ds(0, HD)]), (wv_hbm, wkv.at[pl.ds(HD, HD)]),
                (wq_hbm, wq), (wo_hbm, wo.at[0]),
            ]
        )
    ]
    for copy in copies:
        copy.start()

    barrier = pltpu.get_barrier_semaphore()
    peers = [(sp, right), (sp, left), (sp, far), sibling] + z_peers + y_peers
    for peer in peers:
        pl.semaphore_signal(barrier, inc=1, device_id=peer, device_id_type=MESH)

    sends = []

    def send(src, dst, recv, peer):
        copy = pltpu.make_async_remote_copy(
            src_ref=src, dst_ref=dst, send_sem=send_sem.at[len(sends)], recv_sem=recv,
            device_id=peer, device_id_type=MESH,
        )
        sends.append(copy)
        copy.start()
        return copy

    i2, j2 = rows((128, 128)), lanes((128, 128))
    lower = (j2 & 31) < 16
    perm[...] = jnp.where(
        lower & (i2 == j2 + 16), -1.0, jnp.where((~lower) & (i2 == j2 - 16), 1.0, 0.0)
    ).astype(BF16)
    ones[...] = jnp.where((i2 // 64) == (j2 // 64), 1.0 / 64.0, 0.0).astype(BF16)
    qg = qg_ref[...].astype(F32)
    kg = kg_ref[...].astype(F32)
    lane1 = lanes((8, 128))
    for g in range(3):
        if g < 2:
            pair = jnp.concatenate([qg[2 * g : 2 * g + 1], qg[2 * g + 1 : 2 * g + 2]], axis=1)
            pair = pair * (HD ** (-0.5) * LOG2E)
        else:
            pair = jnp.concatenate([kg, kg], axis=1)
        pair = jnp.broadcast_to(pair, (8, 128))
        gains[2 * g] = pair
        gains[2 * g + 1] = jnp.where((lane1 & 31) < 16, pltpu.roll(pair, 112, 1), pltpu.roll(pair, 16, 1))

    lane = lanes((BLK, 128))
    inside = lane & 63
    exponent = (inside & 15).astype(F32) * (-math.log(10000.0) / 16.0)
    freq = jnp.exp(exponent)

    for s in range(4):
        within = rows((BLK, 128))
        if s == 1:
            place = jnp.where(within < HALF, left * BLK, right * BLK) + within
        elif s == 2:
            place = jnp.where(within < HALF, left * BLK + HALF, right * BLK - HALF) + within
        else:
            place = owner[s] * BLK + within
        place = sp * 384 + place
        grid_row = (place >> 6).astype(F32)
        grid_col = (place & 63).astype(F32)
        angle = jnp.where(inside < 32, grid_row, grid_col) * freq
        turns[0, s], turns[1, s] = jnp.cos(angle), jnp.sin(angle)

    vT[:, HD:VROWS] = jnp.ones((16, VROWS - HD, KC), BF16)
    pl.semaphore_wait(barrier, len(peers))
    copies[0].wait()
    halves = (pl.ds(0, HALF), pl.ds(HALF, HALF))
    tok_r, tok_l = [None, None], [None, None]
    for i in (0, 1):
        tok_r[i] = send(toks.at[0, halves[i]], toks.at[1 + i, halves[0]], tok_sem.at[0, i], (sp, right))
        tok_l[1 - i] = send(
            toks.at[0, halves[1 - i]], toks.at[1 + i, halves[1]], tok_sem.at[1, 1 - i], (sp, left)
        )
    for copy in copies[1:4]:
        copy.wait()

    def prepare(s, raw, g):
        value = raw.astype(F32)
        turned = jnp.dot(raw, perm[...], preferred_element_type=F32)
        square = value * value
        high = square.astype(BF16)
        low = (square - high.astype(F32)).astype(BF16)
        mean = jnp.dot(high, ones[...], preferred_element_type=F32) + jnp.dot(
            low, ones[...], preferred_element_type=F32
        )
        inverse = lax.rsqrt(mean + 1e-6)
        return inverse * (
            value * gains[2 * g, 0:1] * turns[0, s] + turned * gains[2 * g + 1, 0:1] * turns[1, s]
        )

    def project_keys(s):
        raw = lax.dot_general(
            toks[s], wkv[...], (((1,), (1,)), ((), ())), preferred_element_type=F32
        ).astype(BF16)
        slab = jnp.where(lane < 64, prepare(s, raw, 2), raw.astype(F32))
        kv[c, 4 * s + z, y] = slab.astype(BF16)

    def project_queries(s):
        raw = jnp.dot(toks[s], wq[...], preferred_element_type=F32).astype(BF16)
        for g in range(2):
            done = prepare(s, raw[:, 128 * g : 128 * g + 128], g)
            q_rows[s, 2 * g] = jnp.where(lane < 64, done, 0.0).astype(BF16)
            q_rows[s, 2 * g + 1] = jnp.where(lane < 64, pltpu.roll(done, 64, 1), 0.0).astype(BF16)

    def phase1(s):
        a = kv.at[c, 4 * s + z, y, halves[0]]
        b = kv.at[c, 4 * s + z, y, halves[1]]
        first = [send(a, a, p1_sem.at[s, 0, d], z_peers[d]) for d in range(3)]
        return first + [send(b, b, p1_sem.at[s, 1, d], y_peers[d]) for d in range(3)]

    def phase2(s):
        a = kv.at[c, pl.ds(4 * s, 4), y, halves[0]]
        b = kv.at[c, 4 * s + z, :, halves[1]]
        first = [send(a, a, p2_sem.at[s, 0, d], y_peers[d]) for d in range(3)]
        return first + [send(b, b, p2_sem.at[s, 1, d], z_peers[d]) for d in range(3)]

    def share(s):
        a = kv.at[c, pl.ds(4 * s, 4)]
        return [send(a, a, sib_sem.at[s], sibling)]

    def arrive(group):
        for copy in group:
            copy.wait_recv()

    acc[...] = jnp.zeros_like(acc)
    mref[...] = jnp.full_like(mref, -1e30)
    per_tile = QT // STAGE_Q

    def keys_of(i):
        s, r = ORDER[i][1:]
        core = lax.rem(c + r // 2, 2)
        place = 4 * s + 2 * (r % 2)
        return kv[core, place : place + 2].reshape(KC, 128)

    def scores(i, part):
        tile, slot = ORDER[i][0], i % 2
        q = q_rows[tile * per_tile : (tile + 1) * per_tile].reshape(QT, 128)[part]
        s = lax.dot_general(keys_of(i), q, (((1,), (1,)), ((), ())), preferred_element_type=F32)
        sbuf[slot, :, part] = s
        mnew[slot, 0:1, part] = jnp.max(s, axis=0, keepdims=True)

    def weigh(i, part):
        tile, slot = ORDER[i][0], i % 2
        chunk = 4 * ORDER[i][1] + ORDER[i][2]
        if part.start == 0 and ORDER[i][1:] not in [other[1:] for other in ORDER[:i]]:
            flipped = keys_of(i).T
            vT[chunk, 0:HD] = flipped[HD:128]
        for cols in [part]:
            old = mref[tile, 0:1, cols]
            new = jnp.maximum(old, mnew[slot, 0:1, cols])
            weights = jnp.exp2(sbuf[slot, :, cols] - new).astype(BF16)
            factor = jnp.exp2(old - new)
            acc[tile, :, cols] = acc[tile, :, cols] * factor + jnp.dot(
                vT[chunk], weights, preferred_element_type=F32
            )
            mref[tile, 0:1, cols] = new

    def tiles(lo, hi, parts=(0, 1)):
        while lo < hi:
            end = min(lo + 2, hi)

            @pl.when(sp >= 0)
            def _():
                for i in range(lo, end):
                    for j in parts:
                        cols = slice(j * STAGE_Q, (j + 1) * STAGE_Q)
                        if i + 1 < len(ORDER):
                            scores(i + 1, cols)
                        weigh(i, cols)

            lo = end

    def finish(s):
        part = acc[s // 2, :, (s % 2) * STAGE_Q : (s % 2 + 1) * STAGE_Q]
        o = (part[0:HD] / part[HD : HD + 1]).T
        for g in range(2):
            att_buf[s, :, 128 * g : 128 * g + 128] = jnp.concatenate(
                [o[2 * g * BLK : (2 * g + 1) * BLK], o[(2 * g + 1) * BLK : (2 * g + 2) * BLK]], axis=1
            ).astype(BF16)

    project_keys(0)
    one0 = phase1(0)
    project_queries(0)
    arrive(one0)
    two0 = phase2(0)
    arrive([tok_r[0]])
    tok_fr = send(toks.at[1, halves[0]], toks.at[3, halves[0]], tok_sem.at[2, 0], (sp, right))
    arrive([tok_l[1]])
    tok_fl = send(toks.at[1, halves[1]], toks.at[3, halves[1]], tok_sem.at[2, 1], (sp, left))
    project_keys(1)
    one1 = phase1(1)
    project_queries(1)
    arrive(two0)
    sib0 = share(0)
    scores(0, slice(0, QT))
    tiles(0, 1)

    def first_shared():
        arrive(sib0)
        tiles(1, 3)

    pl.when(c == 0)(first_shared)
    arrive(one1)
    two1 = phase2(1)
    arrive([tok_r[1], tok_l[0]])
    project_keys(2)
    one2 = phase1(2)
    project_queries(2)
    pl.when(c == 1)(first_shared)
    arrive([tok_fr, tok_fl])
    copies[4].wait()
    wo_half = OUT_ROWS // 4
    base = c * (OUT_ROWS // 2)
    wparts = [pl.ds(pl.multiple_of(base + k * wo_half, wo_half), wo_half) for k in (0, 1)]
    wo_r, wo_l = [None, None], [None, None]
    for i in (0, 1):
        wo_r[i] = send(wo.at[0, wparts[i]], wo.at[1, wparts[i]], wo_sem.at[0, i], (sp, right))
        wo_l[1 - i] = send(
            wo.at[0, wparts[1 - i]], wo.at[2, wparts[1 - i]], wo_sem.at[1, 1 - i], (sp, left)
        )
    project_keys(3)
    one3 = phase1(3)
    project_queries(3)
    tiles(3, 5)
    arrive(one2)
    two2 = phase2(2)
    arrive(two1)
    sib1 = share(1)
    tiles(5, 7)
    arrive(one3)
    two3 = phase2(3)
    tiles(7, 11)
    arrive(sib1)
    tiles(11, 13)
    arrive(two2)
    sib2 = share(2)
    tiles(13, 17)
    arrive([wo_r[0]])
    wo_fr = send(wo.at[1, wparts[0]], wo.at[3, wparts[0]], wo_sem.at[2, 0], (sp, right))
    arrive([wo_l[1]])
    wo_fl = send(wo.at[2, wparts[1]], wo.at[3, wparts[1]], wo_sem.at[2, 1], (sp, left))
    arrive(two3)
    sib3 = share(3)
    tiles(17, 19)
    arrive(sib2)
    tiles(19, 23)
    tiles(23, 25)
    arrive([wo_r[1], wo_l[0]])
    whole = pl.ds(pl.multiple_of(base, OUT_ROWS // 2), OUT_ROWS // 2)
    wsib = [send(wo.at[k, whole], wo.at[k, whole], wsib_sem.at[k - 1], sibling) for k in (1, 2)]
    arrive(sib3)
    tiles(25, 28)
    finish(2)
    finish(3)

    def hand_over(s, half, slot, into, sem, peer):
        return send(att_buf.at[s, halves[half]], att_in.at[slot, halves[into]], att_sem.at[sem], peer)

    atts = [
        hand_over(2, 0, 0, 1, 0, (sp, left)),
        hand_over(2, 1, 1, 0, 1, (sp, right)),
        send(att_buf.at[3], att_in.at[2], att_sem.at[2], (sp, far)),
    ]
    tiles(28, 32, (1,))
    finish(1)
    atts.append(hand_over(1, 0, 0, 0, 3, (sp, left)))
    atts.append(hand_over(1, 1, 1, 1, 4, (sp, right)))
    arrive([wo_fr, wo_fl])
    wsib.append(send(wo.at[3, whole], wo.at[3, whole], wsib_sem.at[2], sibling))
    tiles(28, 32, (0,))
    finish(0)

    logs = jnp.concatenate(
        [(mref[k, 0:1] + jnp.log2(acc[k, HD : HD + 1])) * LN2 for k in (0, 1)], axis=1
    )
    tall = jnp.broadcast_to(logs, (128, NQ)).T
    places = [
        (0, tp * BLK), (HALF, tp * BLK + HALF), (0, left * BLK), (HALF, right * BLK + HALF),
        (0, left * BLK + HALF), (HALF, right * BLK), (0, far * BLK), (HALF, far * BLK + HALF),
    ]
    for k, (inner, place) in enumerate(places):
        mixed = jnp.zeros((HALF, 128), F32)
        for h in range(HEADS):
            start = (k // 2) * STAGE_Q + h * BLK + inner
            mixed = jnp.where(lane[0:HALF] == h, tall[start : start + HALF], mixed)
        lrows[pl.ds(pl.multiple_of(place, HALF), HALF)] = mixed
    log_ref[...] = lrows[...].T[0:HEADS]
    leaving = [pltpu.make_async_copy(log_ref, log_hbm, local_sem.at[5])]
    leaving[0].start()

    width = 512

    def out_product(value, slot, part, first=False, last=False):
        for n in range(D // width):
            cols = pl.ds(n * width, width)
            product = jnp.dot(value, wo[slot, :, cols], preferred_element_type=F32)
            if not first:
                product = product + total[part, cols]
            if last:
                out_ref[part, cols] = product.astype(BF16)
                leaving.append(
                    pltpu.make_async_copy(
                        out_ref.at[part, cols], out_hbm.at[part, cols], local_sem.at[5 + len(leaving)]
                    )
                )
                leaving[-1].start()
            else:
                total[part, cols] = product

    out_product(att_buf[0], 0, pl.ds(0, BLK), first=True)
    arrive(wsib[0:2])
    arrive(atts[0:2])
    out_product(att_in[1, halves[0]], 1, halves[0])
    out_product(att_in[0, halves[1]], 2, halves[1])
    arrive(wsib[2:3])
    arrive(atts[2:3])
    out_product(att_in[2], 3, pl.ds(0, BLK))
    arrive(atts[3:5])
    out_product(att_in[0, halves[0]], 2, halves[0], last=True)
    out_product(att_in[1, halves[1]], 1, halves[1], last=True)

    for copy in leaving:
        copy.wait()
    for copy in sends:
        copy.wait_send()


def body(tokens, query_weight, key_weight, value_weight, out_weight, query_gain, key_gain):
    any_spec = pl.BlockSpec(memory_space=pl.ANY)
    vmem = pl.BlockSpec(memory_space=pltpu.VMEM)
    dma = pltpu.SemaphoreType.DMA
    return pl.pallas_call(
        kernel,
        out_shape=(
            jax.ShapeDtypeStruct((BLK, D), BF16),
            jax.ShapeDtypeStruct((HEADS, 4 * BLK), F32),
        ),
        in_specs=[any_spec] * 5 + [vmem] * 2,
        out_specs=(any_spec, any_spec),
        scratch_shapes=[
            pltpu.VMEM((4, BLK, D), BF16),
            pltpu.VMEM((D, 256), BF16),
            pltpu.VMEM((128, D), BF16),
            pltpu.VMEM((4, OUT_ROWS, D), BF16),
            pltpu.VMEM((2, 4, BLK, 128), F32),
            pltpu.VMEM((BLK, D), F32),
            pltpu.VMEM((128, 128), BF16),
            pltpu.VMEM((128, 128), BF16),
            pltpu.VMEM((6, 8, 128), F32),
            pltpu.VMEM((4, HEADS, BLK, 128), BF16),
            pltpu.VMEM((NC, 16, NY, BLK, 128), BF16),
            pltpu.VMEM((16, VROWS, KC), BF16),
            pltpu.VMEM((2, KC, QT), F32),
            pltpu.VMEM((2, 8, QT), F32),
            pltpu.VMEM((2, VROWS, QT), F32),
            pltpu.VMEM((2, 8, QT), F32),
            pltpu.VMEM((BLK, D), BF16),
            pltpu.VMEM((HEADS, 4 * BLK), F32),
            pltpu.VMEM((4, BLK, 256), BF16),
            pltpu.VMEM((3, BLK, 256), BF16),
            pltpu.VMEM((4 * BLK, 128), F32),
            dma((14,)),
            dma((80,)),
            dma((3, 2)),
            dma((4, 2, 3)),
            dma((4, 2, 3)),
            dma((4,)),
            dma((3, 2)),
            dma((3,)),
            dma((5,)),
        ],
        compiler_params=pltpu.CompilerParams(
            collective_id=0, has_side_effects=True, vmem_limit_bytes=60 * 2**20
        ),
    )(tokens, query_weight, key_weight.T, value_weight.T, out_weight, query_gain, key_gain)


def solution(mesh):
    return jax.shard_map(
        body,
        mesh=mesh,
        in_specs=(
            P(("sp", "tp"), None),
            P(None, "tp"),
            P(None, "tp"),
            P(None, "tp"),
            P("tp", None),
            P("tp", None),
            P("tp", None),
        ),
        out_specs=(P(("sp", "tp"), None), P("tp", "sp")),
        check_vma=False,
    )
```
